256 devices in a mesh: ep: 128 (over z, y, x), tp: 2 (over core).
Axes of the slice: x: 4, y: 4, z: 8, core: 2. Of those that a mesh axis runs over, the one named last changes fastest.
Arguments:
- tokens: bfloat16 [2048, 2048], P('ep'), may hold values from -6 to 6
- mix_gain: float32 [2048], replicated, may hold values from 0.1 to 1.9
- query_weight: bfloat16 [2048, 1024], P('ep', 'tp'), may hold values from -0.125 to 0.125
- forget_weight: bfloat16 [2048, 1024], P('ep', 'tp'), may hold values from -0.125 to 0.125
- input_weight: bfloat16 [2048, 1024], P('ep', 'tp'), may hold values from -0.125 to 0.125
- lower_bound: float32 [1024], P('tp'), may hold values from 0 to 0.9
- head_gain: float32 [1024], P('tp'), may hold values from 0.1 to 1.9
- out_weight: bfloat16 [1024, 2048], P('tp', 'ep'), may hold values from -0.1875 to 0.1875
- state: float32 [2048, 8, 128, 128], P('ep', 'tp'), may hold values from -4 to 4
- ffn_gain: float32 [2048], replicated, may hold values from 0.1 to 1.9
- route_ids: int32 [2048, 2], P('ep'), may hold values from 0 to 7, all different within a row; in each aligned block of 16 rows (0 to 15, 16 to 31, ...) at most 6 rows name the same one
- route_weights: float32 [2048, 2], P('ep'), may hold values from 0.25 to 1
- expert_gate: bfloat16 [128, 2048, 256], P('ep', None, 'tp'), may hold values from -0.125 to 0.125
- expert_up: bfloat16 [128, 2048, 256], P('ep', None, 'tp'), may hold values from -0.125 to 0.125
- expert_down: bfloat16 [128, 256, 2048], P('ep', 'tp'), may hold values from -0.09375 to 0.09375
Outputs:
- mixed_out: bfloat16 [2048, 2048], P('ep', 'tp')
- new_state: float32 [2048, 8, 128, 128], P('ep', 'tp')
The draws below stay inside these ranges and needn't reach their ends.
Inputs may be any that keep to these rules, and one draw needn't show every extreme that they name: `route_ids`: each row names 2 different experts; among the rows of one device no expert is named by more than 6 rows, a bound that some block reaches of them.
All inputs are finite; a program needn't handle non-finite values.
Results may differ from the reference program's by a relative error of at most 0.015.
Values may be sent and summed in bfloat16 or wider, within the bound.
A program may use at most 64 MiB of HBM per device.

```python
import math
import jax
import jax.numpy as jnp
import numpy as np
from jax import lax

D = 2048
HEADS = 8
HEAD_DIM = 128
FF_E = 4096
EXPERTS = 8
TOP = 2
SEQ_DEV = 16
CAP = 6
SEQS = 2048
SPAN = 16
N_EP = 128
N_TP = 2


def steps_of(own_key, extent, shards, smallest, high):
    def one(position, shards_of):
        steps = jax.random.uniform(jax.random.fold_in(jax.random.fold_in(own_key, 6), position), (shards_of,), jnp.float32, smallest / len(shards), high / len(shards))
        return jnp.repeat(jnp.exp(steps), extent[position] // shards_of).reshape((-1,) + (1,) * (len(extent) - position - 1))

    level = one(*shards[0])
    for cut in shards[1:]:
        level = level * one(*cut)
    return level


def assign_block(own_key, own, number, rows, count, top, bound, slope):
    ranking = jax.random.permutation(own_key, count)
    packed, ordinary = portions_of(count, rows * top, bound, slope, True), portions_of(count, rows * top, bound, slope, False)
    places = jnp.arange(count)

    def named(tallies, rotation):
        used = int((tallies > 0).sum())
        fixed = max(1, used // 4)
        moved = fixed + (places - fixed + rotation * (used - fixed)) % max(1, count - fixed)
        return jnp.zeros((count,), jnp.int32).at[ranking[jnp.where(places < fixed, places, moved)]].set(jnp.asarray(tallies, jnp.int32))

    tallies = jnp.where(number % 4 == 0, named(packed, number // 4), named(ordinary, number - number // 4 - 1))
    mixed = jax.random.permutation(jax.random.fold_in(own, 3), count)
    giver, receiver = mixed[0:count // 2 * 2:2], mixed[1:count // 2 * 2:2]
    margin = jnp.minimum(tallies[giver] - 1, bound - tallies[receiver]) // 2
    margin = jnp.where((giver == ranking[0]) | (receiver == ranking[0]) | (tallies[receiver] == 0), 0, jnp.maximum(margin, 0))
    moved = jax.random.randint(jax.random.fold_in(own, 4), (count // 2,), 0, 1 << 20) % (margin + 1)
    tallies = tallies.at[giver].add(-moved).at[receiver].add(moved)
    labels = jnp.searchsorted(jnp.cumsum(tallies), jnp.arange(rows * top), side="right").astype(jnp.int32)
    grid = labels.reshape(top, rows).T
    grid = grid[jax.random.permutation(jax.random.fold_in(own, 1), rows)]
    rotation = jax.random.randint(jax.random.fold_in(own, 2), (rows, 1), 0, top)
    return jnp.take_along_axis(grid, (jnp.arange(top)[None, :] + rotation) % top, axis=1)


def portions_of(count, total, reach, slope, full):
    weights = [(1 << 20) // math.isqrt(rank ** slope) + 1 for rank in range(1, count + 1)]
    largest = reach if full else min(reach, max(-(-total // count), total * weights[0] // sum(weights)))
    least = 1 if total - largest >= count - 1 else 0
    counts, rest = [largest] + [least] * (count - 1), total - largest - least * (count - 1)
    while rest > 0:
        movable = [i for i in range(1, count) if counts[i] < largest] or [i for i in range(1, count) if counts[i] < reach]
        mass, budget = sum([weights[i] for i in movable]), rest
        for i in movable:
            extra = min(reach - counts[i], max(1, budget * weights[i] // mass), rest)
            counts[i] = counts[i] + extra
            rest = rest - extra
    return np.array(counts)


def centred(own_key, extent, spread, limit, shards=(), held_as=jnp.bfloat16):
    values = spread * jax.random.normal(own_key, extent, jnp.float32)
    if shards:
        values = values * steps_of(own_key, extent, shards, -0.22, 0.18)
    return jnp.clip(values, -limit, limit).astype(held_as)


def setup_inputs(seed: int = 0) -> dict:
    arg_keys = jax.random.split(jax.random.key(seed), 16)
    tokens = centred(arg_keys[0], (SEQS, D), 1.0, 6.0, ((0, 128),))
    mix_gain = jnp.clip(1.0 + 0.18 * jax.random.normal(arg_keys[1], (D,), jnp.float32), 0.1, 1.9)
    query_weight = centred(arg_keys[2], (D, HEADS * HEAD_DIM), D ** -0.5, 0.125, ((0, 128), (1, 2)))
    forget_weight = centred(arg_keys[3], (D, HEADS * HEAD_DIM), D ** -0.5, 0.125, ((0, 128), (1, 2)))
    input_weight = centred(arg_keys[4], (D, HEADS * HEAD_DIM), D ** -0.5, 0.125, ((0, 128), (1, 2)))
    lower_bound = jnp.clip(0.9 * jax.random.uniform(arg_keys[5], (HEADS * HEAD_DIM,), jnp.float32) ** steps_of(arg_keys[5], (HEADS * HEAD_DIM,), ((0, 2),), -0.2, 0.2), 0.0, 0.9)
    head_gain = jnp.clip(1.0 + 0.18 * jax.random.normal(arg_keys[6], (HEADS * HEAD_DIM,), jnp.float32), 0.1, 1.9)
    out_weight = centred(arg_keys[7], (HEADS * HEAD_DIM, D), (HEADS * HEAD_DIM) ** -0.5, 0.1875, ((0, 2), (1, 128)))
    state = centred(arg_keys[8], (SEQS, HEADS, HEAD_DIM, HEAD_DIM), 0.5, 4.0, ((0, 128), (1, 2)), jnp.float32)
    ffn_gain = jnp.clip(1.0 + 0.18 * jax.random.normal(arg_keys[9], (D,), jnp.float32), 0.1, 1.9)
    route_ids_keys = jax.random.split(jax.random.fold_in(arg_keys[10], 1), SEQS // SEQ_DEV)
    route_ids_turns = jax.random.permutation(jax.random.fold_in(arg_keys[10], 3), SEQS // SEQ_DEV)
    route_ids = jax.vmap(lambda own, number: assign_block(jax.random.fold_in(arg_keys[10], 2), own, number, SEQ_DEV, EXPERTS, TOP, CAP, 2))(route_ids_keys, route_ids_turns).reshape((SEQS, TOP))
    route_weights = jnp.clip(0.25 + 0.75 * jax.random.uniform(arg_keys[11], (SEQS, TOP), jnp.float32) ** steps_of(arg_keys[11], (SEQS, TOP), ((0, 128),), -0.2, 0.2), 0.25, 1.0)
    expert_gate = centred(arg_keys[12], (EXPERTS * SPAN, D, FF_E // SPAN), D ** -0.5, 0.125, ((0, 128), (2, 2)))
    expert_up = centred(arg_keys[13], (EXPERTS * SPAN, D, FF_E // SPAN), D ** -0.5, 0.125, ((0, 128), (2, 2)))
    expert_down = centred(arg_keys[14], (EXPERTS * SPAN, FF_E // SPAN, D), FF_E ** -0.5, 0.09375, ((0, 128), (1, 2)))
    return {"tokens": tokens, "mix_gain": mix_gain, "query_weight": query_weight, "forget_weight": forget_weight, "input_weight": input_weight, "lower_bound": lower_bound, "head_gain": head_gain, "out_weight": out_weight, "state": state, "ffn_gain": ffn_gain, "route_ids": route_ids, "route_weights": route_weights, "expert_gate": expert_gate, "expert_up": expert_up, "expert_down": expert_down}


epsilon = 1e-06

def rms_scale(values_in, gain_vec):
    return values_in * lax.rsqrt(lax.optimization_barrier(jnp.mean(values_in * values_in, axis=-1, keepdims=True)) + epsilon) * gain_vec

def reference(tokens, mix_gain, query_weight, forget_weight, input_weight, lower_bound, head_gain, out_weight, state, ffn_gain, route_ids, route_weights, expert_gate, expert_up, expert_down):
    batch_size = tokens.shape[0]
    residual = tokens.astype(jnp.float32)
    normed = rms_scale(residual, mix_gain).astype(jnp.bfloat16)
    queries = jnp.dot(normed, query_weight, preferred_element_type=jnp.float32).reshape(batch_size, HEADS, HEAD_DIM)
    forget_pre = jnp.dot(normed, forget_weight, preferred_element_type=jnp.float32)
    fresh_values = jnp.dot(normed, input_weight, preferred_element_type=jnp.float32).reshape(batch_size, HEADS, HEAD_DIM)
    forget = (lower_bound + (1.0 - lower_bound) * jax.nn.sigmoid(forget_pre)).reshape(batch_size, HEADS, HEAD_DIM)
    new_state = forget[..., None] * state + (1.0 - forget)[..., None] * fresh_values[:, :, None, :]
    readout = jnp.einsum('shk,shkv->shv', queries, new_state, precision=lax.Precision.HIGHEST)
    readout = rms_scale(readout, head_gain.reshape(HEADS, HEAD_DIM))
    heads_out = readout.reshape(batch_size, HEADS * HEAD_DIM).astype(jnp.bfloat16)
    group_cols = HEADS * HEAD_DIM // N_TP
    mixer_sum = jnp.zeros((batch_size, D), jnp.float32)
    for group in range(N_TP):
        product = jnp.dot(heads_out[:, group * group_cols:(group + 1) * group_cols], out_weight[group * group_cols:(group + 1) * group_cols], preferred_element_type=jnp.float32).astype(jnp.bfloat16)
        product = lax.optimization_barrier(product)
        mixer_sum = mixer_sum + product.astype(jnp.float32)
    after_mixer = (residual + mixer_sum).astype(jnp.bfloat16)
    ffn_in = rms_scale(after_mixer.astype(jnp.float32), ffn_gain).astype(jnp.bfloat16)
    expert_span = N_EP // EXPERTS
    span_cols = FF_E // expert_span
    gate_full = expert_gate.reshape(EXPERTS, expert_span, D, span_cols).transpose(0, 2, 1, 3).reshape(EXPERTS, D, FF_E)
    up_full = expert_up.reshape(EXPERTS, expert_span, D, span_cols).transpose(0, 2, 1, 3).reshape(EXPERTS, D, FF_E)
    down_full = expert_down.reshape(EXPERTS, FF_E, D)
    pair_count = SEQ_DEV * TOP
    flat_ids = route_ids.reshape(N_EP, pair_count).astype(jnp.int32)
    onehot = (flat_ids[..., None] == jnp.arange(EXPERTS, dtype=jnp.int32)).astype(jnp.int32)
    slot_rank = lax.optimization_barrier(jnp.sum((jnp.cumsum(onehot, axis=1).astype(jnp.int32) - onehot) * onehot, axis=-1)).astype(jnp.int32)
    slot_index = (jnp.arange(N_EP, dtype=jnp.int32)[:, None] * CAP + slot_rank).reshape(-1).astype(jnp.int32)
    expert_index = flat_ids.reshape(-1)
    token_index = (jnp.arange(batch_size * TOP, dtype=jnp.int32) // TOP).astype(jnp.int32)
    slot_table = jnp.full((EXPERTS, N_EP * CAP), batch_size, dtype=jnp.int32).at[expert_index, slot_index].set(token_index)
    padded_rows = jnp.concatenate([ffn_in, jnp.zeros((1, D), jnp.bfloat16)], axis=0)

    def expert_step(inputs):
        gate_w, up_w, down_w, table_row = inputs
        slot_rows = padded_rows[table_row]
        gate_pre = jnp.dot(slot_rows, gate_w, preferred_element_type=jnp.float32)
        up_pre = jnp.dot(slot_rows, up_w, preferred_element_type=jnp.float32)
        hidden = (jax.nn.silu(gate_pre) * up_pre).astype(jnp.bfloat16)
        return jnp.dot(hidden, down_w, preferred_element_type=jnp.float32)
    expert_out = lax.map(expert_step, (gate_full, up_full, down_full, slot_table))
    picked = expert_out[expert_index, slot_index].reshape(batch_size, TOP, D)
    expert_mix = lax.optimization_barrier(jnp.sum(picked * route_weights[:, :, None], axis=1))
    mixed_out = (after_mixer.astype(jnp.float32) + expert_mix).astype(jnp.bfloat16)
    return (mixed_out, new_state)
```

```python
import functools
import jax
import jax.numpy as jnp
from jax import lax
from jax.experimental import pallas as pl
from jax.experimental.pallas import tpu as pltpu
from jax.sharding import Mesh
from jax.sharding import PartitionSpec as P

EXPERTS = 8
TOP = 2
EP = ("z", "y", "x")
MESH_ID = pl.DeviceIdType.MESH
F32 = jnp.float32
BF16 = jnp.bfloat16
epsilon = 1e-06


def place():
    c, z = lax.axis_index("tp"), lax.axis_index("z")
    y, x = lax.axis_index("y"), lax.axis_index("x")
    first = c == 0
    return c, z, y, x, jnp.where(first, x, y), jnp.where(first, y, x)


def plane_id(c, u, v):
    first = c == 0
    return {"x": jnp.where(first, u, v), "y": jnp.where(first, v, u)}


def remote(src, dst, send, recv, device):
    return pltpu.make_async_remote_copy(
        src_ref=src, dst_ref=dst, send_sem=send, recv_sem=recv, device_id=device, device_id_type=MESH_ID
    )


def arrived(ref, sem):
    pltpu.make_async_copy(ref, ref, sem).wait()


def route_slots(ids_ref, wts_ref):
    row = lax.broadcasted_iota(jnp.int32, (64, 16), 0)
    expert, slot = row // 8, row % 8
    pick0 = (jnp.broadcast_to(ids_ref[0:1, :], (64, 16)) == expert).astype(F32)
    pick1 = (jnp.broadcast_to(ids_ref[1:2, :], (64, 16)) == expert).astype(F32)
    pick = pick0 + pick1
    earlier = (
        lax.broadcasted_iota(jnp.int32, (16, 16), 0) < lax.broadcasted_iota(jnp.int32, (16, 16), 1)
    ).astype(F32)
    rank = jnp.dot(pick, earlier, preferred_element_type=F32)
    chosen = jnp.where(rank == slot.astype(F32), pick, 0.0)
    weight = pick0 * jnp.broadcast_to(wts_ref[0:1, :], (64, 16)) + pick1 * jnp.broadcast_to(wts_ref[1:2, :], (64, 16))
    return chosen, chosen * weight


def squeeze_rows():
    to = lax.broadcasted_iota(jnp.int32, (24, 32), 0)
    frm = lax.broadcasted_iota(jnp.int32, (24, 32), 1)
    return (((to // 6) * 8 + to % 6) == frm).astype(BF16)


def spread_rows():
    to = lax.broadcasted_iota(jnp.int32, (32, 24), 0)
    frm = lax.broadcasted_iota(jnp.int32, (32, 24), 1)
    return (((frm // 6) * 8 + frm % 6) == to).astype(BF16)


def moe_kernel(
    am_ref, gain_ref, ids_ref, wts_ref, gate_ref, up_ref, down_ref, out_ref,
    wgu, wd, disp, zr, xg, po, r1, ss, r2, ret, rb,
    wsem, wsend, wrecv, dsend, drecv, gsend, grecv, psend, precv, ssend, srecv, tsend, trecv,
):
    c, z, y, x, u, v = place()
    half = am_ref.shape[1] // 2
    mine = lax.rem(z, 2) == c
    other = 1 - c
    bar = pltpu.get_barrier_semaphore()
    peers = [{"tp": other}]
    for k in range(1, 8):
        zk = lax.rem(z + k, 8)
        peers += [{"z": zk}, {"z": zk, "tp": other}]
    for k in range(1, 4):
        peers += [plane_id(c, lax.rem(u + k, 4), v), plane_id(c, u, lax.rem(v + k, 4))]
    for device in peers:
        pl.semaphore_signal(bar, inc=1, device_id=device, device_id_type=MESH_ID)
    own = pl.ds(pl.multiple_of(c * 128, 128), 128)
    own_up = pl.ds(pl.multiple_of(256 + c * 128, 128), 128)
    local = [
        pltpu.make_async_copy(gate_ref.at[0], wgu.at[:, own], wsem.at[0]),
        pltpu.make_async_copy(up_ref.at[0], wgu.at[:, own_up], wsem.at[1]),
        pltpu.make_async_copy(down_ref.at[0], wd.at[own, :], wsem.at[2]),
    ]
    for copy in local:
        copy.start()
    rows = am_ref[...].astype(F32)
    scale = lax.rsqrt(jnp.mean(rows * rows, axis=-1, keepdims=True) + epsilon)
    ffn_in = (rows * scale * gain_ref[...]).astype(BF16)
    chosen, weight = route_slots(ids_ref, wts_ref)
    slots = jnp.dot(chosen.astype(BF16), ffn_in, preferred_element_type=F32).astype(BF16)
    disp[...] = slots.reshape(disp.shape)
    pl.semaphore_wait(bar, len(peers))
    swap = [
        remote(gate_ref.at[0], wgu.at[:, own], wsend.at[0], wrecv.at[0], {"tp": other}),
        remote(up_ref.at[0], wgu.at[:, own_up], wsend.at[1], wrecv.at[1], {"tp": other}),
        remote(down_ref.at[0], wd.at[own, :], wsend.at[2], wrecv.at[2], {"tp": other}),
    ]
    sends = []
    for k in (4, 3, 5, 2, 6, 1, 7):
        e = lax.rem(z + k, 8)
        copy = remote(disp.at[e], zr.at[z // 2], dsend.at[k], drecv.at[z // 2], {"z": e})

        @pl.when(mine)
        def _(copy=copy):
            copy.start()

    for copy in swap:
        copy.start()
    for k in range(4):

        @pl.when(2 * k + c != z)
        def _(k=k):
            arrived(zr.at[k], drecv.at[k])

    @pl.when(mine)
    def _():
        zr[z // 2] = disp[z]

    packed = jnp.dot(squeeze_rows(), zr[...].reshape(32, 2 * half), preferred_element_type=F32).astype(BF16)
    home = v * 4 + u
    xg[home] = packed
    number = 0

    def share(block, device):
        nonlocal number
        copy = remote(xg.at[block], xg.at[block], gsend.at[number], grecv.at[block], device)
        copy.start()
        sends.append(copy)
        number += 1

    for k in (2, 1, 3):
        share(home, plane_id(c, lax.rem(u + k, 4), v))
    for k in (2, 1, 3):
        share(home, plane_id(c, u, lax.rem(v + k, 4)))
    for k in (1, 3, 2):
        block = v * 4 + lax.rem(u + k, 4)
        arrived(xg.at[block], grecv.at[block])
        for j in (2, 1, 3):
            share(block, plane_id(c, u, lax.rem(v + j, 4)))
    for copy in local:
        copy.wait()
    for copy in swap:
        copy.wait_recv()

    def group(step, carry):
        vv = lax.rem(v + step, 4)
        base = pl.multiple_of(vv * 4, 4)

        @pl.when(step > 0)
        def _():
            for j in range(4):
                arrived(xg.at[base + j], grecv.at[base + j])

        lhs = xg[pl.ds(base, 4)].reshape(96, 2 * half)
        pre = jnp.dot(lhs, wgu[...], preferred_element_type=F32)
        gate_pre, up_pre = pre[:, :256], pre[:, 256:]
        hidden = (gate_pre / (1.0 + jnp.exp(-gate_pre)) * up_pre).astype(BF16)
        part = jnp.dot(hidden, wd[...], preferred_element_type=F32).astype(BF16)
        po[vv] = part.reshape(4, 24, 2 * half)

        @pl.when(step > 0)
        def _():
            remote(po.at[vv], r1.at[v], psend.at[vv], precv.at[v], plane_id(c, u, vv)).start()

        return carry

    lax.fori_loop(0, 4, group, 0)
    for k in (1, 3, 2):
        vk = lax.rem(v + k, 4)
        arrived(r1.at[vk], precv.at[vk])
    for k in (2, 1, 3, 0):
        uk = lax.rem(u + k, 4)
        total = po[v, uk].astype(F32)
        for j in (1, 2, 3):
            total += r1[lax.rem(v + j, 4), uk].astype(F32)
        if k:
            ss[uk] = total.astype(BF16)
            remote(ss.at[uk], r2.at[u], ssend.at[k], srecv.at[u], plane_id(c, uk, v)).start()
    for k in (1, 3, 2):
        uk = lax.rem(u + k, 4)
        arrived(r2.at[uk], srecv.at[uk])
        total += r2[uk].astype(F32)
    ret[...] = (
        jnp.dot(spread_rows(), total.astype(BF16), preferred_element_type=F32).astype(BF16).reshape(ret.shape)
    )
    for k in range(4):
        zk = 2 * k + c
        for t in range(2):
            piece = ret.at[k, :, pl.ds(t * half, half)]
            copy = remote(piece, rb.at[z], tsend.at[k, t], trecv.at[z], {"z": zk, "tp": t})

            @pl.when(jnp.logical_or(zk != z, c != t))
            def _(copy=copy):
                copy.start()

    @pl.when(mine)
    def _():
        rb[z] = ret[z // 2, :, pl.ds(pl.multiple_of(c * half, half), half)]

    for k in (1, 7, 2, 6, 3, 5, 4):
        e = lax.rem(z + k, 8)
        arrived(rb.at[e], trecv.at[e])

    @pl.when(jnp.logical_not(mine))
    def _():
        arrived(rb.at[z], trecv.at[z])

    returned = rb[...].reshape(64, half)
    upper = weight.astype(BF16)
    lower = (weight - upper.astype(F32)).astype(BF16)
    dims = (((0,), (0,)), ((), ()))
    mix = lax.dot_general(upper, returned, dims, preferred_element_type=F32)
    mix += lax.dot_general(lower, returned, dims, preferred_element_type=F32)
    keep = am_ref[:, pl.ds(pl.multiple_of(c * half, half), half)].astype(F32)
    out_ref[...] = (keep + mix).astype(BF16)
    for k in (4, 3, 5, 2, 6, 1, 7):

        @pl.when(mine)
        def _(k=k):
            arrived(disp.at[0], dsend.at[k])

    for copy in swap:
        copy.wait_send()
    for copy in sends:
        copy.wait_send()
    for k in (1, 2, 3):
        vk = lax.rem(v + k, 4)
        arrived(po.at[vk], psend.at[vk])
        arrived(ss.at[0], ssend.at[k])
    for k in range(4):
        for t in range(2):

            @pl.when(jnp.logical_or(2 * k + c != z, c != t))
            def _(k=k, t=t):
                arrived(rb.at[0], tsend.at[k, t])


def experts(after_mixer, ffn_gain, route_ids, route_weights, expert_gate, expert_up, expert_down):
    rows, width = after_mixer.shape
    half = width // 2
    vmem = pl.BlockSpec(memory_space=pltpu.VMEM)
    hbm = pl.BlockSpec(memory_space=pltpu.HBM)
    dma = pltpu.SemaphoreType.DMA
    return pl.pallas_call(
        moe_kernel,
        out_shape=jax.ShapeDtypeStruct((rows, half), BF16),
        in_specs=[vmem, vmem, vmem, vmem, hbm, hbm, hbm],
        out_specs=vmem,
        scratch_shapes=[
            pltpu.VMEM((width, 512), BF16),
            pltpu.VMEM((256, width), BF16),
            pltpu.VMEM((8, 8, width), BF16),
            pltpu.VMEM((4, 8, width), BF16),
            pltpu.VMEM((16, 24, width), BF16),
            pltpu.VMEM((4, 4, 24, width), BF16),
            pltpu.VMEM((4, 4, 24, width), BF16),
            pltpu.VMEM((4, 24, width), BF16),
            pltpu.VMEM((4, 24, width), BF16),
            pltpu.VMEM((4, 8, width), BF16),
            pltpu.VMEM((8, 8, half), BF16),
            dma((3,)), dma((3,)), dma((3,)),
            dma((8,)), dma((4,)),
            dma((15,)), dma((16,)),
            dma((4,)), dma((4,)),
            dma((4,)), dma((4,)),
            dma((4, 2)), dma((8,)),
        ],
        compiler_params=pltpu.CompilerParams(
            collective_id=3, has_side_effects=True, vmem_limit_bytes=40 * 2**20
        ),
        name="experts",
    )(
        after_mixer, ffn_gain.reshape(1, -1), route_ids.T, route_weights.T, expert_gate, expert_up, expert_down
    )


def side_by_side(arrays, axis, dim, along):
    both = jnp.concatenate(arrays, axis=along)
    filled, at, done = (lax.all_gather(both, axis, axis=dim, tiled=True), 0, [])
    for a in arrays:
        done.append(lax.slice_in_dim(filled, at, at + a.shape[along], axis=along))
        at += a.shape[along]
    return tuple(done)


def gathered_by_axis(shard, axes, dim):
    for axis in reversed(axes):
        shard = lax.all_gather(shard, axis, axis=dim, tiled=True)
    return shard


def sent_to_all(shard, axis):
    copies = jnp.broadcast_to(shard, (lax.axis_size(axis), *shard.shape))
    return lax.all_to_all(copies, axis, split_axis=0, concat_axis=0, tiled=True)


def over_copies(shard, axis):
    everything = sent_to_all(shard, axis)
    return jnp.sum(everything.astype(jnp.float32), axis=0)


def cut_along(shard, dim, peers):
    before, after = (shard.shape[:dim], shard.shape[dim + 1 :])
    return jnp.moveaxis(shard.reshape(*before, peers, -1, *after), dim, 0)


def summed_on_arrival(shard, axis, dim):
    parts = cut_along(shard, dim, lax.axis_size(axis))
    arrived = lax.all_to_all(parts, axis, split_axis=0, concat_axis=0, tiled=True)
    return arrived.astype(jnp.float32).sum(axis=0)


def rms_scale(values_in, gain_vec):
    return (
        values_in
        * lax.rsqrt(jnp.mean(values_in * values_in, axis=-1, keepdims=True) + epsilon)
        * gain_vec
    )


def shards(
    tokens,
    mix_gain,
    query_weight,
    forget_weight,
    input_weight,
    lower_bound,
    head_gain,
    out_weight,
    state,
    ffn_gain,
    route_ids,
    route_weights,
    expert_gate,
    expert_up,
    expert_down,
):
    seq_dev = tokens.shape[0]
    model_width = tokens.shape[1]
    ep_count = lax.axis_size(EP)
    residual = tokens.astype(jnp.float32)
    normed = rms_scale(residual, mix_gain).astype(jnp.bfloat16)
    head_count = state.shape[1]
    head_size = state.shape[2]
    proj_width = query_weight.shape[1]
    pieces = side_by_side((query_weight, forget_weight, input_weight), EP, 0, 1)
    queries, forget_pre, fresh_values = tuple(
        (jnp.dot(normed, weight_rows, preferred_element_type=jnp.float32) for weight_rows in pieces)
    )
    forget = (lower_bound + (1.0 - lower_bound) * jax.nn.sigmoid(forget_pre)).reshape(
        seq_dev, head_count, head_size
    )
    queries = queries.reshape(seq_dev, head_count, head_size)
    fresh_values = fresh_values.reshape(seq_dev, head_count, head_size)
    new_state = forget[..., None] * state + (1.0 - forget)[..., None] * fresh_values[:, :, None, :]
    readout = jnp.einsum("shk,shkv->shv", queries, new_state, precision=lax.Precision.HIGHEST)
    readout = rms_scale(readout, head_gain.reshape(head_count, head_size))
    heads_out = readout.reshape(seq_dev, proj_width).astype(jnp.bfloat16)
    partial_mix = jnp.dot(
        heads_out, gathered_by_axis(out_weight, EP, 1), preferred_element_type=jnp.float32
    )
    mixer_sum = over_copies(partial_mix.astype(jnp.bfloat16), "tp").astype(jnp.float32)
    after_mixer = (residual + mixer_sum).astype(jnp.bfloat16)
    mixed_out = experts(after_mixer, ffn_gain, route_ids, route_weights, expert_gate, expert_up, expert_down)
    return (mixed_out, new_state)


def solution(mesh):
    finer = Mesh(mesh.devices.reshape(8, 4, 4, mesh.shape["tp"]), ("z", "y", "x", "tp"))
    placed = (
        P(EP, None),
        P(),
        P(EP, "tp"),
        P(EP, "tp"),
        P(EP, "tp"),
        P("tp"),
        P("tp"),
        P("tp", EP),
        P(EP, "tp", None, None),
        P(),
        P(EP, None),
        P(EP, None),
        P(EP, None, "tp"),
        P(EP, None, "tp"),
        P(EP, "tp", None),
    )
    return jax.shard_map(
        shards,
        mesh=finer,
        in_specs=placed,
        out_specs=(P(EP, "tp"), P(EP, "tp", None, None)),
        check_vma=False,
    )
```

```python
import functools
import jax
import jax.numpy as jnp
from jax import lax
from jax.experimental import pallas as pl
from jax.experimental.pallas import tpu as pltpu
from jax.sharding import Mesh
from jax.sharding import PartitionSpec as P

EXPERTS = 8
TOP = 2
EP = ("z", "y", "x")
MESH_ID = pl.DeviceIdType.MESH
F32 = jnp.float32
BF16 = jnp.bfloat16
epsilon = 1e-06


def place():
    c, z = lax.axis_index("tp"), lax.axis_index("z")
    y, x = lax.axis_index("y"), lax.axis_index("x")
    first = c == 0
    return c, z, y, x, jnp.where(first, x, y), jnp.where(first, y, x)


def plane_id(c, u, v):
    first = c == 0
    return {"x": jnp.where(first, u, v), "y": jnp.where(first, v, u)}


def remote(src, dst, send, recv, device):
    return pltpu.make_async_remote_copy(
        src_ref=src, dst_ref=dst, send_sem=send, recv_sem=recv, device_id=device, device_id_type=MESH_ID
    )


def arrived(ref, sem):
    pltpu.make_async_copy(ref, ref, sem).wait()


def route_slots(ids_ref, wts_ref):
    row = lax.broadcasted_iota(jnp.int32, (64, 16), 0)
    expert, slot = row // 8, row % 8
    pick0 = (jnp.broadcast_to(ids_ref[0:1, :], (64, 16)) == expert).astype(F32)
    pick1 = (jnp.broadcast_to(ids_ref[1:2, :], (64, 16)) == expert).astype(F32)
    pick = pick0 + pick1
    earlier = (
        lax.broadcasted_iota(jnp.int32, (16, 16), 0) < lax.broadcasted_iota(jnp.int32, (16, 16), 1)
    ).astype(F32)
    rank = jnp.dot(pick, earlier, preferred_element_type=F32)
    chosen = jnp.where(rank == slot.astype(F32), pick, 0.0)
    weight = pick0 * jnp.broadcast_to(wts_ref[0:1, :], (64, 16)) + pick1 * jnp.broadcast_to(wts_ref[1:2, :], (64, 16))
    return chosen, chosen * weight


def squeeze_rows():
    to = lax.broadcasted_iota(jnp.int32, (24, 32), 0)
    frm = lax.broadcasted_iota(jnp.int32, (24, 32), 1)
    return (((to // 6) * 8 + to % 6) == frm).astype(BF16)


def spread_rows():
    to = lax.broadcasted_iota(jnp.int32, (32, 24), 0)
    frm = lax.broadcasted_iota(jnp.int32, (32, 24), 1)
    return (((frm // 6) * 8 + frm % 6) == to).astype(BF16)


def halves(left, right, odd):
    lane = lax.broadcasted_iota(jnp.int32, left.shape, 1)
    if odd:
        left = pltpu.roll(left, 64, 1)
    else:
        right = pltpu.roll(right, 64, 1)
    return jnp.where(lane < 64, left, right)


def layer_kernel(
    tok_hbm, mixg_hbm, qw_hbm, fw_hbm, iw_hbm, lb_hbm, hg_hbm, wo_hbm, st_hbm, ffng_hbm, ids_hbm, wts_hbm,
    gate_ref, up_ref, down_ref, out_ref, st,
    tok, mixg, lb, hg, ffng, ids_ref, wts_ref, wcat, wb, xs, xb, ob, qb, ro, ho, wob, hb, pb, mb, am_ref, chosen_ref, weight_ref,
    wgu, wd, disp, zr, xg, po, r1, ss, r2, ret, rb,
    lsem, qsem, stsem, wsend, wrecv, xsend, xrecv, osend, orecv, wozs, wozr, woxs, woxr, hsend, hrecv, msend, mrecv,
    lwsem, swsend, swrecv, dsend, drecv, gsend, grecv, psend, precv, ssend, srecv, tsend, trecv,
):
    c, z, y, x, u, v = place()
    half = out_ref.shape[1]
    mine = lax.rem(z, 2) == c
    other = 1 - c
    spot = y * 4 + x
    bar = pltpu.get_barrier_semaphore()
    peers = [{"tp": other}]
    for dz in range(8):
        zk = lax.rem(z + dz, 8)
        for dx in range(4):
            if dz or dx:
                peers.append({"z": zk, "x": lax.rem(x + dx, 4)})
        if dz:
            peers.append({"z": zk, "tp": other})
    for dy in range(1, 4):
        yk = lax.rem(y + dy, 4)
        for dx in range(4):
            peers.append({"y": yk, "x": lax.rem(x + dx, 4)})
        peers.append({"y": yk, "tp": other})
    for device in peers:
        pl.semaphore_signal(bar, inc=1, device_id=device, device_id_type=MESH_ID)
    loads = [
        pltpu.make_async_copy(a, b, lsem.at[i])
        for i, (a, b) in enumerate(
            ((tok_hbm, tok), (mixg_hbm, mixg), (lb_hbm, lb), (hg_hbm, hg), (ffng_hbm, ffng), (ids_hbm, ids_ref), (wts_hbm, wts_ref),
             (wo_hbm, wob.at[z, x]))
        )
    ]
    own = pl.ds(pl.multiple_of(c * 128, 128), 128)
    own_up = pl.ds(pl.multiple_of(256 + c * 128, 128), 128)
    pieces = []
    for i, w_hbm in enumerate((qw_hbm, fw_hbm, iw_hbm)):
        for h in range(4):
            pieces.append(
                pltpu.make_async_copy(w_hbm.at[:, pl.ds(h * 128, 128)], wcat.at[h, :, pl.ds(i * 128, 128)], qsem.at[i, h])
            )
    for copy in loads[:2] + pieces + loads[2:]:
        copy.start()
    local = [
        pltpu.make_async_copy(gate_ref.at[0], wgu.at[:, own], lwsem.at[0]),
        pltpu.make_async_copy(up_ref.at[0], wgu.at[:, own_up], lwsem.at[1]),
        pltpu.make_async_copy(down_ref.at[0], wd.at[own, :], lwsem.at[2]),
    ]
    state_in = pltpu.make_async_copy(st_hbm, st, stsem)
    state_in.start()
    for copy in local:
        copy.start()
    for copy in loads[:2]:
        copy.wait()
    tokens = tok[...].astype(F32)
    scale = lax.rsqrt(jnp.mean(tokens * tokens, axis=-1, keepdims=True) + epsilon)
    normed = tokens * scale * mixg[...]
    for yk in range(4):
        for j in range(4):
            a, b = 4 * j + yk // 2, 4 * j + 2 + yk // 2
            xs[yk, :, pl.ds(j * 128, 128)] = halves(
                normed[:, a * 128 : a * 128 + 128], normed[:, b * 128 : b * 128 + 128], yk % 2
            ).astype(BF16)
    for copy in pieces:
        copy.wait()
    pl.semaphore_wait(bar, len(peers))
    out = []
    for dz in (4, 3, 5, 2, 6, 1, 7, 0):
        for dx in (2, 1, 3, 0):
            if dz or dx:
                xk = lax.rem(x + dx, 4)
                out.append(remote(wcat.at[xk], wb.at[z, x], wsend.at[dz, dx], wrecv, {"z": lax.rem(z + dz, 8), "x": xk}))
    for dy in (2, 1, 3, 0):
        for dx in (2, 1, 3, 0):
            if dy or dx:
                yk = lax.rem(y + dy, 4)
                out.append(remote(xs.at[yk], xb.at[spot], xsend.at[dy, dx], xrecv, {"y": yk, "x": lax.rem(x + dx, 4)}))
    for copy in out:
        copy.start()
    wb[z, x] = wcat[x]
    xb[spot] = xs[y]
    for copy in loads[2:]:
        copy.wait()
    spread = []
    for k in (4, 3, 5, 2, 6, 1, 7):
        spread.append(remote(wob.at[z, x], wob.at[z, x], wozs.at[k], wozr, {"z": lax.rem(z + k, 8)}))
    for copy in spread:
        copy.start()
    swap = [
        remote(gate_ref.at[0], wgu.at[:, own], swsend.at[0], swrecv.at[0], {"tp": other}),
        remote(up_ref.at[0], wgu.at[:, own_up], swsend.at[1], swrecv.at[1], {"tp": other}),
        remote(down_ref.at[0], wd.at[own, :], swsend.at[2], swrecv.at[2], {"tp": other}),
    ]
    for copy in swap:
        copy.start()
    chosen, weight = route_slots(ids_ref, wts_ref)
    chosen_ref[...] = chosen.astype(BF16)
    weight_ref[...] = weight
    arrived(xb.at[pl.ds(0, 15)], xrecv)
    wbf = wb.reshape(32, 16, 384)
    arrived(wbf.at[pl.ds(0, 31)], wrecv)
    part = jnp.dot(xb[...].reshape(256, 512), wbf[...].reshape(512, 384), preferred_element_type=F32)
    ob[...] = part.astype(BF16).reshape(16, 16, 384)
    back = []
    for dy in (2, 1, 3, 0):
        for dx in (2, 1, 3, 0):
            if dy or dx:
                yk, xk = lax.rem(y + dy, 4), lax.rem(x + dx, 4)
                back.append(remote(ob.at[yk * 4 + xk], qb.at[spot], osend.at[dy, dx], orecv, {"y": yk, "x": xk}))
    for copy in back:
        copy.start()
    qb[spot] = ob[spot]
    arrived(xb.at[pl.ds(0, 7)], wozr)
    along = []
    for k in (2, 1, 3):
        along.append(remote(wob.at[:, x], wob.at[:, x], woxs.at[k], woxr, {"x": lax.rem(x + k, 4)}))
    for copy in along:
        copy.start()
    state_in.wait()
    arrived(qb.at[pl.ds(0, 15)], orecv)

    def head(h, carry):
        qfv = (
            qb[h].astype(F32) + qb[4 + h].astype(F32) + qb[8 + h].astype(F32) + qb[12 + h].astype(F32)
        )
        bound = lb[pl.ds(h, 1), :]
        forget = bound + (1.0 - bound) * (1.0 / (1.0 + jnp.exp(-qfv[:, 128:256])))
        fresh = qfv[:, 256:384]
        q_t = qfv[:, 0:128].T
        f_t = forget.T
        for s in range(16):
            f_col = jnp.broadcast_to(f_t[:, s : s + 1], (128, 128))
            q_col = jnp.broadcast_to(q_t[:, s : s + 1], (128, 128))
            row = fresh[s : s + 1, :]
            new = row + f_col * (st[s, h] - row)
            st[s, h] = new
            ro[s : s + 1, :] = jnp.sum(q_col * new, axis=0, keepdims=True)
        read = ro[...]
        read = read * lax.rsqrt(jnp.mean(read * read, axis=-1, keepdims=True) + epsilon) * hg[pl.ds(h, 1), :]
        ho[:, pl.ds(pl.multiple_of(h * 128, 128), 128)] = read.astype(BF16)
        return carry

    lax.fori_loop(0, 4, head, 0)
    ahead = []
    for k in (2, 1, 3):
        ahead.append(remote(ho, hb.at[y], hsend.at[k], hrecv, {"y": lax.rem(y + k, 4)}))
    for copy in ahead:
        copy.start()
    hb[y] = ho[...]
    arrived(wob.at[:, pl.ds(0, 3)], woxr)
    arrived(hb.at[pl.ds(0, 3)], hrecv)
    dims = (((1,), (1,)), ((), ()))
    mixed = lax.dot_general(
        hb[...].reshape(64, 512), wob[...].reshape(512, 512), dims, preferred_element_type=F32
    )
    pb[...] = mixed.astype(BF16).reshape(4, 16, 512)
    home_bound = []
    for k in (2, 1, 3, 0):
        yk = lax.rem(y + k, 4)
        for t in (0, 1):
            if k or t:
                device = {"y": yk, "tp": lax.rem(c + t, 2)}
                home_bound.append(remote(pb.at[yk], mb.at[c, y], msend.at[k, t], mrecv, device))
    for copy in home_bound:
        copy.start()
    mb[c, y] = pb[y]
    arrived(mb.reshape(8, 16, 512).at[pl.ds(0, 7)], mrecv)
    sums = [mb[0, k].astype(F32) + mb[1, k].astype(F32) for k in range(4)]
    for zk in range(8):
        at = (zk // 2) * 128
        for h in range(2):
            cols = pl.ds(zk * 256 + h * 128, 128)
            got = halves(sums[2 * h][:, at : at + 128], sums[2 * h + 1][:, at : at + 128], zk % 2)
            am_ref[:, cols] = (tok[:, cols].astype(F32) + got).astype(BF16)
    rows = am_ref[...].astype(F32)
    scale = lax.rsqrt(jnp.mean(rows * rows, axis=-1, keepdims=True) + epsilon)
    ffn_in = (rows * scale * ffng[...]).astype(BF16)
    slots = jnp.dot(chosen_ref[...], ffn_in, preferred_element_type=F32).astype(BF16)
    disp[...] = slots.reshape(disp.shape)
    sends = []
    for k in (4, 3, 5, 2, 6, 1, 7):
        e = lax.rem(z + k, 8)
        copy = remote(disp.at[e], zr.at[z // 2], dsend.at[k], drecv.at[z // 2], {"z": e})

        @pl.when(mine)
        def _(copy=copy):
            copy.start()

    for k in range(4):

        @pl.when(2 * k + c != z)
        def _(k=k):
            arrived(zr.at[k], drecv.at[k])

    @pl.when(mine)
    def _():
        zr[z // 2] = disp[z]

    packed = jnp.dot(squeeze_rows(), zr[...].reshape(32, 2 * half), preferred_element_type=F32).astype(BF16)
    home = v * 4 + u
    xg[home] = packed
    number = 0

    def share(block, device):
        nonlocal number
        copy = remote(xg.at[block], xg.at[block], gsend.at[number], grecv.at[block], device)
        copy.start()
        sends.append(copy)
        number += 1

    for k in (2, 1, 3):
        share(home, plane_id(c, lax.rem(u + k, 4), v))
    for k in (2, 1, 3):
        share(home, plane_id(c, u, lax.rem(v + k, 4)))
    for k in (1, 3, 2):
        block = v * 4 + lax.rem(u + k, 4)
        arrived(xg.at[block], grecv.at[block])
        for j in (2, 1, 3):
            share(block, plane_id(c, u, lax.rem(v + j, 4)))
    for copy in local:
        copy.wait()
    for copy in swap:
        copy.wait_recv()

    def group(step, carry):
        vv = lax.rem(v + step, 4)
        base = pl.multiple_of(vv * 4, 4)

        @pl.when(step > 0)
        def _():
            for j in range(4):
                arrived(xg.at[base + j], grecv.at[base + j])

        lhs = xg[pl.ds(base, 4)].reshape(96, 2 * half)
        pre = jnp.dot(lhs, wgu[...], preferred_element_type=F32)
        gate_pre, up_pre = pre[:, :256], pre[:, 256:]
        hidden = (gate_pre / (1.0 + jnp.exp(-gate_pre)) * up_pre).astype(BF16)
        part = jnp.dot(hidden, wd[...], preferred_element_type=F32).astype(BF16)
        po[vv] = part.reshape(4, 24, 2 * half)

        @pl.when(step > 0)
        def _():
            remote(po.at[vv], r1.at[v], psend.at[vv], precv.at[v], plane_id(c, u, vv)).start()

        return carry

    lax.fori_loop(0, 4, group, 0)
    for k in (1, 3, 2):
        vk = lax.rem(v + k, 4)
        arrived(r1.at[vk], precv.at[vk])
    for k in (2, 1, 3, 0):
        uk = lax.rem(u + k, 4)
        total = po[v, uk].astype(F32)
        for j in (1, 2, 3):
            total += r1[lax.rem(v + j, 4), uk].astype(F32)
        if k:
            ss[uk] = total.astype(BF16)
            remote(ss.at[uk], r2.at[u], ssend.at[k], srecv.at[u], plane_id(c, uk, v)).start()
    for k in (1, 3, 2):
        uk = lax.rem(u + k, 4)
        arrived(r2.at[uk], srecv.at[uk])
        total += r2[uk].astype(F32)
    ret[...] = (
        jnp.dot(spread_rows(), total.astype(BF16), preferred_element_type=F32).astype(BF16).reshape(ret.shape)
    )
    for k in range(4):
        zk = 2 * k + c
        for t in range(2):
            piece = ret.at[k, :, pl.ds(t * half, half)]
            copy = remote(piece, rb.at[z], tsend.at[k, t], trecv.at[z], {"z": zk, "tp": t})

            @pl.when(jnp.logical_or(zk != z, c != t))
            def _(copy=copy):
                copy.start()

    @pl.when(mine)
    def _():
        rb[z] = ret[z // 2, :, pl.ds(pl.multiple_of(c * half, half), half)]

    for k in (1, 7, 2, 6, 3, 5, 4):
        e = lax.rem(z + k, 8)
        arrived(rb.at[e], trecv.at[e])

    @pl.when(jnp.logical_not(mine))
    def _():
        arrived(rb.at[z], trecv.at[z])

    returned = rb[...].reshape(64, half)
    weight = weight_ref[...]
    upper = weight.astype(BF16)
    lower = (weight - upper.astype(F32)).astype(BF16)
    dims = (((0,), (0,)), ((), ()))
    mix = lax.dot_general(upper, returned, dims, preferred_element_type=F32)
    mix += lax.dot_general(lower, returned, dims, preferred_element_type=F32)
    keep = am_ref[:, pl.ds(pl.multiple_of(c * half, half), half)].astype(F32)
    out_ref[...] = (keep + mix).astype(BF16)
    for k in (4, 3, 5, 2, 6, 1, 7):

        @pl.when(mine)
        def _(k=k):
            arrived(disp.at[0], dsend.at[k])

    for copy in swap:
        copy.wait_send()
    for copy in sends:
        copy.wait_send()
    for k in (1, 2, 3):
        vk = lax.rem(v + k, 4)
        arrived(po.at[vk], psend.at[vk])
        arrived(ss.at[0], ssend.at[k])
    for k in range(4):
        for t in range(2):

            @pl.when(jnp.logical_or(2 * k + c != z, c != t))
            def _(k=k, t=t):
                arrived(rb.at[0], tsend.at[k, t])
    for copy in out + spread + back + along + ahead + home_bound:
        copy.wait_send()


def shards(
    tokens, mix_gain, query_weight, forget_weight, input_weight, lower_bound, head_gain, out_weight, state,
    ffn_gain, route_ids, route_weights, expert_gate, expert_up, expert_down,
):
    rows, width = tokens.shape
    half = width // 2
    hbm = pl.BlockSpec(memory_space=pltpu.HBM)
    vmem = pl.BlockSpec(memory_space=pltpu.VMEM)
    dma = pltpu.SemaphoreType.DMA
    scratch = lambda *shape, dtype=BF16: pltpu.VMEM(shape, dtype)
    held = lambda a: pltpu.with_memory_space_constraint(a, pltpu.HBM)
    return pl.pallas_call(
        layer_kernel,
        out_shape=(jax.ShapeDtypeStruct((rows, half), BF16), pltpu.VMEM(state.shape, F32)),
        in_specs=[hbm] * 15,
        out_specs=(vmem, vmem),
        scratch_shapes=[
            scratch(rows, width), scratch(1, width, dtype=F32), scratch(4, 128, dtype=F32), scratch(4, 128, dtype=F32),
            scratch(1, width, dtype=F32), scratch(2, 16, dtype=jnp.int32), scratch(2, 16, dtype=F32),
            scratch(4, 16, 384), scratch(8, 4, 16, 384), scratch(4, 16, 512), scratch(16, 16, 512),
            scratch(16, 16, 384), scratch(16, 16, 384), scratch(16, 128, dtype=F32),
            scratch(16, 512), scratch(8, 4, 16, 512), scratch(4, 16, 512), scratch(4, 16, 512), scratch(2, 4, 16, 512),
            scratch(rows, width), scratch(64, 16), scratch(64, 16, dtype=F32),
            scratch(width, 512), scratch(256, width), scratch(8, 8, width), scratch(4, 8, width),
            scratch(16, 24, width), scratch(4, 4, 24, width), scratch(4, 4, 24, width), scratch(4, 24, width),
            scratch(4, 24, width), scratch(4, 8, width), scratch(8, 8, half),
            dma((8,)), dma((3, 4)), dma, dma((8, 4)), dma, dma((4, 4)), dma, dma((4, 4)), dma,
            dma((8,)), dma, dma((4,)), dma, dma((4,)), dma, dma((4, 2)), dma,
            dma((3,)), dma((3,)), dma((3,)), dma((8,)), dma((4,)), dma((15,)), dma((16,)), dma((4,)), dma((4,)),
            dma((4,)), dma((4,)), dma((4, 2)), dma((8,)),
        ],
        compiler_params=pltpu.CompilerParams(
            collective_id=0, has_side_effects=True, vmem_limit_bytes=48 * 2**20
        ),
        name="layer",
    )(
        *map(held, (
            tokens, mix_gain.reshape(1, -1), query_weight, forget_weight, input_weight, lower_bound.reshape(4, 128),
            head_gain.reshape(4, 128), out_weight.T, state, ffn_gain.reshape(1, -1), route_ids.T, route_weights.T,
            expert_gate, expert_up, expert_down,
        ))
    )


def solution(mesh):
    finer = Mesh(mesh.devices.reshape(8, 4, 4, mesh.shape["tp"]), ("z", "y", "x", "tp"))
    placed = (
        P(EP, None), P(), P(EP, "tp"), P(EP, "tp"), P(EP, "tp"), P("tp"), P("tp"), P("tp", EP),
        P(EP, "tp", None, None), P(), P(EP, None), P(EP, None), P(EP, None, "tp"), P(EP, None, "tp"), P(EP, "tp", None),
    )
    return jax.shard_map(
        shards, mesh=finer, in_specs=placed, out_specs=(P(EP, "tp"), P(EP, "tp", None, None)), check_vma=False
    )
```

```python
import functools
import jax
import jax.numpy as jnp
from jax import lax
from jax.experimental import pallas as pl
from jax.experimental.pallas import tpu as pltpu
from jax.sharding import Mesh
from jax.sharding import PartitionSpec as P

EXPERTS = 8
TOP = 2
EP = ("z", "y", "x")
MESH_ID = pl.DeviceIdType.MESH
F32 = jnp.float32
BF16 = jnp.bfloat16
epsilon = 1e-06
FILLED = 6


def place():
    c, z = lax.axis_index("tp"), lax.axis_index("z")
    y, x = lax.axis_index("y"), lax.axis_index("x")
    first = c == 0
    return c, z, y, x, jnp.where(first, x, y), jnp.where(first, y, x)


def plane_id(c, u, v):
    first = c == 0
    return {"x": jnp.where(first, u, v), "y": jnp.where(first, v, u)}


def remote(src, dst, send, recv, device):
    return pltpu.make_async_remote_copy(
        src_ref=src, dst_ref=dst, send_sem=send, recv_sem=recv, device_id=device, device_id_type=MESH_ID
    )


def arrived(ref, sem):
    pltpu.make_async_copy(ref, ref, sem).wait()


def route_slots(ids_ref, wts_ref):
    row = lax.broadcasted_iota(jnp.int32, (64, 16), 0)
    expert, slot = row // 8, row % 8
    pick0 = (jnp.broadcast_to(ids_ref[0:1, :], (64, 16)) == expert).astype(F32)
    pick1 = (jnp.broadcast_to(ids_ref[1:2, :], (64, 16)) == expert).astype(F32)
    pick = pick0 + pick1
    earlier = (
        lax.broadcasted_iota(jnp.int32, (16, 16), 0) < lax.broadcasted_iota(jnp.int32, (16, 16), 1)
    ).astype(F32)
    rank = jnp.dot(pick, earlier, preferred_element_type=F32)
    chosen = jnp.where(rank == slot.astype(F32), pick, 0.0)
    weight = pick0 * jnp.broadcast_to(wts_ref[0:1, :], (64, 16)) + pick1 * jnp.broadcast_to(wts_ref[1:2, :], (64, 16))
    return chosen, chosen * weight


def squeeze_rows():
    to = lax.broadcasted_iota(jnp.int32, (24, 32), 0)
    frm = lax.broadcasted_iota(jnp.int32, (24, 32), 1)
    return (((to // 6) * 8 + to % 6) == frm).astype(BF16)


def spread_rows():
    to = lax.broadcasted_iota(jnp.int32, (32, 24), 0)
    frm = lax.broadcasted_iota(jnp.int32, (32, 24), 1)
    return (((frm // 6) * 8 + frm % 6) == to).astype(BF16)


def halves(left, right, odd):
    lane = lax.broadcasted_iota(jnp.int32, left.shape, 1)
    if odd:
        left = pltpu.roll(left, 64, 1)
    else:
        right = pltpu.roll(right, 64, 1)
    return jnp.where(lane < 64, left, right)


class Ledger:
    def __init__(self):
        self.open = {}
        self.seen = set()

    def expect(self, key, wait):
        self.open[key] = wait
        self.seen.add(key)

    def wait(self, *keys):
        for key in keys:
            self.open.pop(key)()

    def finish(self):
        for wait in self.open.values():
            wait()
        self.open = {}


def only(condition, do):
    return lambda: pl.when(condition)(do)


def either(condition, these, others, sem):
    def wait():
        pl.when(condition)(lambda: arrived(these, sem))
        pl.when(jnp.logical_not(condition))(lambda: arrived(others, sem))

    return wait


def layer_kernel(
    tok_hbm, mixg_hbm, qw_hbm, fw_hbm, iw_hbm, lb_hbm, hg_hbm, wo_hbm, st_hbm, ffng_hbm, ids_hbm, wts_hbm,
    gate_ref, up_ref, down_ref, out_ref, st,
    tok, mixg, lb, hg, ffng, ids_ref, wts_ref, wcat, wb, xs, xb, ob, qb, ro, ho, wob, hb, pb, mb, am_ref, chosen_ref, weight_ref,
    wgu, wd, disp, zr, xg, po, pr, ss, r2, ret, rb,
    lsem, qsem, stsem, wsend, wrecv, xsend, xrecv, osend, orecv, wozs, wozr, woxs, woxr, hsend, hrecv, msend, mrecv,
    lwsem, swsend, swrecv, dsend, drecv, gsend, gu, gv, psend, precv, ssend, srecv, tsend, trecv,
):
    c, z, y, x, u, v = place()
    half = out_ref.shape[1]
    mine = lax.rem(z, 2) == c
    other = 1 - c
    spot = y * 4 + x
    bar = pltpu.get_barrier_semaphore()
    peers = [{"tp": other}]
    for dz in range(8):
        zk = lax.rem(z + dz, 8)
        for dx in range(4):
            if dz or dx:
                peers.append({"z": zk, "x": lax.rem(x + dx, 4)})
        if dz:
            peers.append({"z": zk, "tp": other})
    for dy in range(1, 4):
        yk = lax.rem(y + dy, 4)
        for dx in range(4):
            peers.append({"y": yk, "x": lax.rem(x + dx, 4)})
        peers.append({"y": yk, "tp": other})
    for device in peers:
        pl.semaphore_signal(bar, inc=1, device_id=device, device_id_type=MESH_ID)
    loads = [
        pltpu.make_async_copy(a, b, lsem.at[i])
        for i, (a, b) in enumerate(
            ((tok_hbm, tok), (mixg_hbm, mixg), (lb_hbm, lb), (hg_hbm, hg), (ffng_hbm, ffng), (ids_hbm, ids_ref), (wts_hbm, wts_ref),
             (wo_hbm, wob.at[z, x]))
        )
    ]
    own = pl.ds(pl.multiple_of(c * 128, 128), 128)
    own_up = pl.ds(pl.multiple_of(256 + c * 128, 128), 128)
    pieces = []
    for i, w_hbm in enumerate((qw_hbm, fw_hbm, iw_hbm)):
        for h in range(4):
            pieces.append(
                pltpu.make_async_copy(w_hbm.at[:, pl.ds(h * 128, 128)], wcat.at[h, :, pl.ds(i * 128, 128)], qsem)
            )
    led = Ledger()
    for i, copy in enumerate(loads[:2] + pieces + loads[2:]):
        copy.start()
    for i, copy in enumerate(loads):
        led.expect(("load", i), copy.wait)
    led.expect("pieces", lambda: arrived(wcat, qsem))
    local = [
        pltpu.make_async_copy(gate_ref.at[0], wgu.at[:, own], lwsem),
        pltpu.make_async_copy(up_ref.at[0], wgu.at[:, own_up], lwsem),
        pltpu.make_async_copy(down_ref.at[0], wd.at[own, :], lwsem),
    ]
    state_in = pltpu.make_async_copy(st_hbm, st, stsem)
    state_in.start()
    led.expect("state", state_in.wait)
    for copy in local:
        copy.start()
    led.expect("local", lambda: arrived(wgu.at[:, pl.ds(0, 384)], lwsem))
    led.wait(("load", 0), ("load", 1))
    tokens = tok[...].astype(F32)
    scale = lax.rsqrt(jnp.mean(tokens * tokens, axis=-1, keepdims=True) + epsilon)
    normed = tokens * scale * mixg[...]
    for yk in range(4):
        for j in range(4):
            a, b = 4 * j + yk // 2, 4 * j + 2 + yk // 2
            xs[yk, :, pl.ds(j * 128, 128)] = halves(
                normed[:, a * 128 : a * 128 + 128], normed[:, b * 128 : b * 128 + 128], yk % 2
            ).astype(BF16)
    led.wait("pieces")
    zr[...] = jnp.zeros_like(zr)
    rb[...] = jnp.zeros_like(rb)
    pl.semaphore_wait(bar, len(peers))
    out = []
    for dz in (4, 3, 5, 2, 6, 1, 7, 0):
        for dx in (2, 1, 3, 0):
            if dz or dx:
                xk = lax.rem(x + dx, 4)
                out.append(remote(wcat.at[xk], wb.at[z, x], wsend, wrecv, {"z": lax.rem(z + dz, 8), "x": xk}))
    for dy in (2, 1, 3, 0):
        for dx in (2, 1, 3, 0):
            if dy or dx:
                yk = lax.rem(y + dy, 4)
                out.append(remote(xs.at[yk], xb.at[spot], xsend, xrecv, {"y": yk, "x": lax.rem(x + dx, 4)}))
    for copy in out:
        copy.start()
    wbf = wb.reshape(32, 16, 384)
    led.expect("x out", lambda: arrived(xb.at[pl.ds(0, 15)], xsend))
    led.expect("w out", lambda: arrived(wbf.at[pl.ds(0, 31)], wsend))
    led.expect("x", lambda: arrived(xb.at[pl.ds(0, 15)], xrecv))
    led.expect("w", lambda: arrived(wbf.at[pl.ds(0, 31)], wrecv))
    wb[z, x] = wcat[x]
    xb[spot] = xs[y]
    led.wait(*(("load", i) for i in range(2, 8)))
    spread = []
    for k in (4, 3, 5, 2, 6, 1, 7):
        spread.append(remote(wob.at[z, x], wob.at[z, x], wozs, wozr, {"z": lax.rem(z + k, 8)}))
    for copy in spread:
        copy.start()
    led.expect("woz out", lambda: arrived(xb.at[pl.ds(0, 7)], wozs))
    led.expect("woz", lambda: arrived(xb.at[pl.ds(0, 7)], wozr))
    swap = [
        remote(gate_ref.at[0], wgu.at[:, own], swsend, swrecv, {"tp": other}),
        remote(up_ref.at[0], wgu.at[:, own_up], swsend, swrecv, {"tp": other}),
        remote(down_ref.at[0], wd.at[own, :], swsend, swrecv, {"tp": other}),
    ]
    for copy in swap:
        copy.start()
    led.expect("swap out", lambda: arrived(wgu.at[:, pl.ds(0, 384)], swsend))
    led.expect("swap in", lambda: arrived(wgu.at[:, pl.ds(0, 384)], swrecv))
    chosen, weight = route_slots(ids_ref, wts_ref)
    chosen_ref[...] = chosen.astype(BF16)
    weight_ref[...] = weight
    led.wait("x", "w")
    part = jnp.dot(xb[...].reshape(256, 512), wbf[...].reshape(512, 384), preferred_element_type=F32)
    ob[...] = part.astype(BF16).reshape(16, 16, 384)
    back = []
    for dy in (2, 1, 3, 0):
        for dx in (2, 1, 3, 0):
            if dy or dx:
                yk, xk = lax.rem(y + dy, 4), lax.rem(x + dx, 4)
                back.append(remote(ob.at[yk * 4 + xk], qb.at[spot], osend, orecv, {"y": yk, "x": xk}))
    for copy in back:
        copy.start()
    led.expect("q out", lambda: arrived(qb.at[pl.ds(0, 15)], osend))
    led.expect("q", lambda: arrived(qb.at[pl.ds(0, 15)], orecv))
    qb[spot] = ob[spot]
    led.wait("woz")
    along = []
    for k in (2, 1, 3):
        along.append(remote(wob.at[:, x], wob.at[:, x], woxs, woxr, {"x": lax.rem(x + k, 4)}))
    for copy in along:
        copy.start()
    led.expect("wox out", lambda: arrived(wob.at[:, pl.ds(0, 3)], woxs))
    led.expect("wox", lambda: arrived(wob.at[:, pl.ds(0, 3)], woxr))
    led.wait("state", "q")

    def head(h, carry):
        qfv = (
            qb[h].astype(F32) + qb[4 + h].astype(F32) + qb[8 + h].astype(F32) + qb[12 + h].astype(F32)
        )
        bound = lb[pl.ds(h, 1), :]
        forget = bound + (1.0 - bound) * (1.0 / (1.0 + jnp.exp(-qfv[:, 128:256])))
        fresh = qfv[:, 256:384]
        q_t = qfv[:, 0:128].T
        f_t = forget.T
        for s in range(16):
            f_col = jnp.broadcast_to(f_t[:, s : s + 1], (128, 128))
            q_col = jnp.broadcast_to(q_t[:, s : s + 1], (128, 128))
            row = fresh[s : s + 1, :]
            new = row + f_col * (st[s, h] - row)
            st[s, h] = new
            ro[s : s + 1, :] = jnp.sum(q_col * new, axis=0, keepdims=True)
        read = ro[...]
        read = read * lax.rsqrt(jnp.mean(read * read, axis=-1, keepdims=True) + epsilon) * hg[pl.ds(h, 1), :]
        ho[:, pl.ds(pl.multiple_of(h * 128, 128), 128)] = read.astype(BF16)
        return carry

    lax.fori_loop(0, 4, head, 0)
    ahead = []
    for k in (2, 1, 3):
        ahead.append(remote(ho, hb.at[y], hsend, hrecv, {"y": lax.rem(y + k, 4)}))
    for copy in ahead:
        copy.start()
    led.expect("h out", lambda: arrived(hb.at[pl.ds(0, 3)], hsend))
    led.expect("h", lambda: arrived(hb.at[pl.ds(0, 3)], hrecv))
    hb[y] = ho[...]
    led.wait("wox", "h")
    dims = (((1,), (1,)), ((), ()))
    mixed = lax.dot_general(
        hb[...].reshape(64, 512), wob[...].reshape(512, 512), dims, preferred_element_type=F32
    )
    pb[...] = mixed.astype(BF16).reshape(4, 16, 512)
    home_bound = []
    for k in (2, 1, 3, 0):
        yk = lax.rem(y + k, 4)
        for t in (0, 1):
            if k or t:
                device = {"y": yk, "tp": lax.rem(c + t, 2)}
                home_bound.append(remote(pb.at[yk], mb.at[c, y], msend, mrecv, device))
    for copy in home_bound:
        copy.start()
    led.expect("m out", lambda: arrived(mb.reshape(8, 16, 512).at[pl.ds(0, 7)], msend))
    led.expect("m", lambda: arrived(mb.reshape(8, 16, 512).at[pl.ds(0, 7)], mrecv))
    mb[c, y] = pb[y]
    led.wait("m")
    sums = [mb[0, k].astype(F32) + mb[1, k].astype(F32) for k in range(4)]
    for zk in range(8):
        at = (zk // 2) * 128
        for h in range(2):
            cols = pl.ds(zk * 256 + h * 128, 128)
            got = halves(sums[2 * h][:, at : at + 128], sums[2 * h + 1][:, at : at + 128], zk % 2)
            am_ref[:, cols] = (tok[:, cols].astype(F32) + got).astype(BF16)
    rows = am_ref[...].astype(F32)
    scale = lax.rsqrt(jnp.mean(rows * rows, axis=-1, keepdims=True) + epsilon)
    ffn_in = (rows * scale * ffng[...]).astype(BF16)
    slots = jnp.dot(chosen_ref[...], ffn_in, preferred_element_type=F32).astype(BF16)
    disp[...] = slots.reshape(disp.shape)
    halves_at = [pl.ds(w * half, half) for w in range(2)]
    for w in range(2):
        for k in (4, 3, 5, 2, 6, 1, 7):
            e = lax.rem(z + k, 8)
            piece = disp.at[e, pl.ds(0, FILLED), halves_at[w]]
            copy = remote(piece, zr.at[w, z // 2, pl.ds(0, FILLED)], dsend, drecv.at[w], {"z": e})

            @pl.when(mine)
            def _(copy=copy):
                copy.start()

        led.expect(("slots", w), either(mine, zr.at[w, pl.ds(0, 3), pl.ds(0, FILLED)], zr.at[w, :, pl.ds(0, FILLED)], drecv.at[w]))
    led.expect("slots out", only(mine, lambda: arrived(disp.at[pl.ds(0, 7), pl.ds(0, FILLED)], dsend)))

    @pl.when(mine)
    def _():
        for w in range(2):
            zr[w, z // 2] = disp[z, :, halves_at[w]]

    lines = [lax.rem(u + j, 4) for j in range(4)]
    across = [lax.rem(v + k, 4) for k in range(4)]
    for w in range(2):
        for j in range(4):
            uj = lines[j]
            if j:
                led.expect(("rows", w, j, 0), lambda w=w, uj=uj: arrived(xg.at[w * 16 + uj * 4 + v], gu.at[w, uj]))
            led.expect(("rows", w, j, 1), lambda w=w, uj=uj: arrived(xg.at[pl.ds(0, 3)], gv.at[w, uj]))
    led.expect("rows out", lambda: arrived(xg.at[pl.ds(0, 30)], gsend))
    led.expect("parts out", lambda: arrived(xg.at[pl.ds(0, 24)], psend))
    led.expect("sums out", lambda: arrived(xg.at[pl.ds(0, 6)], ssend))

    def along_v(w, j):
        block = xg.at[w * 16 + lines[j] * 4 + v]
        for k in (2, 1, 3):
            remote(block, block, gsend, gv.at[w, lines[j]], plane_id(c, u, across[k])).start()

    def from_z(w):
        led.wait(("slots", w))
        packed = jnp.dot(squeeze_rows(), zr[w].reshape(32, half), preferred_element_type=F32).astype(BF16)
        xg[w * 16 + u * 4 + v] = packed
        block = xg.at[w * 16 + u * 4 + v]
        for k in (2, 1, 3):
            remote(block, block, gsend, gu.at[w, u], plane_id(c, lines[k], v)).start()
        along_v(w, 0)

    def from_u(w, j):
        led.wait(("rows", w, j, 0))
        along_v(w, j)

    def first(w, j):
        led.wait(("rows", w, j, 1))
        rows_in = xg[pl.ds(w * 16 + lines[j] * 4, 4)].reshape(96, half)
        return jnp.dot(rows_in, wgu[halves_at[w], :], preferred_element_type=F32)

    def second(j):
        uj = lines[j]
        pre = first(0, j) + first(1, j)
        gate_pre, up_pre = pre[:, :256], pre[:, 256:]
        hidden = (gate_pre / (1.0 + jnp.exp(-gate_pre)) * up_pre).astype(BF16)
        for w in range(2):
            part = jnp.dot(hidden, wd[:, halves_at[w]], preferred_element_type=F32).astype(BF16)
            po[w, uj] = part.reshape(4, 24, half)
            for k in (2, 1, 3):
                there = plane_id(c, u, across[k])
                remote(po.at[w, uj, across[k]], pr.at[w, uj, v], psend, precv.at[w, uj], there).start()
            led.expect(("part in", w, j), lambda w=w: arrived(pr.at[w, uj, pl.ds(0, 3)], precv.at[w, uj]))

    def gather(w, j):
        uj = lines[j]
        led.wait(("part in", w, j))
        total = po[w, uj, v].astype(F32)
        for k in (1, 3, 2):
            total += pr[w, uj, across[k]].astype(F32)
        return total

    def hand_over(w, j):
        uj = lines[j]
        ss[w, uj] = gather(w, j).astype(BF16)
        remote(ss.at[w, uj], r2.at[w, u], ssend, srecv.at[w], plane_id(c, uj, v)).start()

    def give_back(w):
        total = gather(w, 0)
        arrived(r2.at[w, pl.ds(0, 3)], srecv.at[w])
        for k in (1, 3, 2):
            total += r2[w, lines[k]].astype(F32)
        ret[:, :, halves_at[w]] = (
            jnp.dot(spread_rows(), total.astype(BF16), preferred_element_type=F32).astype(BF16).reshape(4, 8, half)
        )
        for k in (2, 1, 3, 0):
            at = lax.rem(z // 2 + k, 4)
            zk = 2 * at + c
            piece = ret.at[at, pl.ds(0, FILLED), halves_at[w]]
            copy = remote(piece, rb.at[z, pl.ds(0, FILLED)], tsend, trecv, {"z": zk, "tp": w})
            away = jnp.logical_or(zk != z, c != w)

            @pl.when(away)
            def _(copy=copy):
                copy.start()


    from_z(0)
    from_z(1)
    led.wait("local", "swap in")
    from_u(0, 3)
    from_u(0, 1)
    from_u(0, 2)
    from_u(1, 3)
    from_u(1, 1)
    from_u(1, 2)
    second(0)
    second(3)
    second(1)
    second(2)
    for j in (3, 1, 2):
        for w in range(2):
            hand_over(w, j)
    give_back(0)
    give_back(1)

    @pl.when(mine)
    def _():
        rb[z] = ret[z // 2, :, pl.ds(pl.multiple_of(c * half, half), half)]

    seven, eight = rb.at[pl.ds(0, 7), pl.ds(0, FILLED)], rb.at[:, pl.ds(0, FILLED)]
    either(mine, seven, eight, trecv)()
    led.expect("returned out", either(mine, seven, eight, tsend))
    returned = rb[...].reshape(64, half)
    weight = weight_ref[...]
    upper = weight.astype(BF16)
    lower = (weight - upper.astype(F32)).astype(BF16)
    dims = (((0,), (0,)), ((), ()))
    mix = lax.dot_general(upper, returned, dims, preferred_element_type=F32)
    mix += lax.dot_general(lower, returned, dims, preferred_element_type=F32)
    keep = am_ref[:, pl.ds(pl.multiple_of(c * half, half), half)].astype(F32)
    out_ref[...] = (keep + mix).astype(BF16)
    led.finish()


def shards(
    tokens, mix_gain, query_weight, forget_weight, input_weight, lower_bound, head_gain, out_weight, state,
    ffn_gain, route_ids, route_weights, expert_gate, expert_up, expert_down,
):
    rows, width = tokens.shape
    half = width // 2
    hbm = pl.BlockSpec(memory_space=pltpu.HBM)
    vmem = pl.BlockSpec(memory_space=pltpu.VMEM)
    dma = pltpu.SemaphoreType.DMA
    scratch = lambda *shape, dtype=BF16: pltpu.VMEM(shape, dtype)
    held = lambda a: pltpu.with_memory_space_constraint(a, pltpu.HBM)
    return pl.pallas_call(
        layer_kernel,
        out_shape=(jax.ShapeDtypeStruct((rows, half), BF16), pltpu.VMEM(state.shape, F32)),
        in_specs=[hbm] * 15,
        out_specs=(vmem, vmem),
        scratch_shapes=[
            scratch(rows, width), scratch(1, width, dtype=F32), scratch(4, 128, dtype=F32), scratch(4, 128, dtype=F32),
            scratch(1, width, dtype=F32), scratch(2, 16, dtype=jnp.int32), scratch(2, 16, dtype=F32),
            scratch(4, 16, 384), scratch(8, 4, 16, 384), scratch(4, 16, 512), scratch(16, 16, 512),
            scratch(16, 16, 384), scratch(16, 16, 384), scratch(16, 128, dtype=F32),
            scratch(16, 512), scratch(8, 4, 16, 512), scratch(4, 16, 512), scratch(4, 16, 512), scratch(2, 4, 16, 512),
            scratch(rows, width), scratch(64, 16), scratch(64, 16, dtype=F32),
            scratch(width, 512), scratch(256, width), scratch(8, 8, width), scratch(2, 4, 8, half),
            scratch(32, 24, half), scratch(2, 4, 4, 24, half), scratch(2, 4, 4, 24, half), scratch(2, 4, 24, half),
            scratch(2, 4, 24, half),
            scratch(4, 8, width), scratch(8, 8, half),
            dma((8,)), *[dma] * 16,
            *[dma] * 3, dma, dma((2,)), dma, dma((2, 4)), dma((2, 4)), dma, dma((2, 4)), dma, dma((2,)), dma, dma,
        ],
        compiler_params=pltpu.CompilerParams(
            collective_id=0, has_side_effects=True, vmem_limit_bytes=48 * 2**20
        ),
        name="layer",
    )(
        *map(held, (
            tokens, mix_gain.reshape(1, -1), query_weight, forget_weight, input_weight, lower_bound.reshape(4, 128),
            head_gain.reshape(4, 128), out_weight.T, state, ffn_gain.reshape(1, -1), route_ids.T, route_weights.T,
            expert_gate, expert_up, expert_down,
        ))
    )


def solution(mesh):
    finer = Mesh(mesh.devices.reshape(8, 4, 4, mesh.shape["tp"]), ("z", "y", "x", "tp"))
    placed = (
        P(EP, None), P(), P(EP, "tp"), P(EP, "tp"), P(EP, "tp"), P("tp"), P("tp"), P("tp", EP),
        P(EP, "tp", None, None), P(), P(EP, None), P(EP, None), P(EP, None, "tp"), P(EP, None, "tp"), P(EP, "tp", None),
    )
    return jax.shard_map(
        shards, mesh=finer, in_specs=placed, out_specs=(P(EP, "tp"), P(EP, "tp", None, None)), check_vma=False
    )
```

```python
import functools
import jax
import jax.numpy as jnp
from jax import lax
from jax.experimental import pallas as pl
from jax.experimental.pallas import tpu as pltpu
from jax.sharding import Mesh
from jax.sharding import PartitionSpec as P

EXPERTS = 8
TOP = 2
EP = ("z", "y", "x")
MESH_ID = pl.DeviceIdType.MESH
F32 = jnp.float32
BF16 = jnp.bfloat16
epsilon = 1e-06
FILLED = 6


def place():
    c, z = lax.axis_index("tp"), lax.axis_index("z")
    y, x = lax.axis_index("y"), lax.axis_index("x")
    first = c == 0
    return c, z, y, x, jnp.where(first, x, y), jnp.where(first, y, x)


def plane_id(c, u, v):
    first = c == 0
    return {"x": jnp.where(first, u, v), "y": jnp.where(first, v, u)}


def remote(src, dst, send, recv, device):
    return pltpu.make_async_remote_copy(
        src_ref=src, dst_ref=dst, send_sem=send, recv_sem=recv, device_id=device, device_id_type=MESH_ID
    )


def arrived(ref, sem):
    pltpu.make_async_copy(ref, ref, sem).wait()


def route_slots(ids_ref, wts_ref):
    row = lax.broadcasted_iota(jnp.int32, (64, 16), 0)
    expert, slot = row // 8, row % 8
    pick0 = (jnp.broadcast_to(ids_ref[0:1, :], (64, 16)) == expert).astype(F32)
    pick1 = (jnp.broadcast_to(ids_ref[1:2, :], (64, 16)) == expert).astype(F32)
    pick = pick0 + pick1
    earlier = (
        lax.broadcasted_iota(jnp.int32, (16, 16), 0) < lax.broadcasted_iota(jnp.int32, (16, 16), 1)
    ).astype(F32)
    rank = jnp.dot(pick, earlier, preferred_element_type=F32)
    chosen = jnp.where(rank == slot.astype(F32), pick, 0.0)
    weight = pick0 * jnp.broadcast_to(wts_ref[0:1, :], (64, 16)) + pick1 * jnp.broadcast_to(wts_ref[1:2, :], (64, 16))
    return chosen, chosen * weight


def squeeze_rows():
    to = lax.broadcasted_iota(jnp.int32, (24, 32), 0)
    frm = lax.broadcasted_iota(jnp.int32, (24, 32), 1)
    return (((to // 6) * 8 + to % 6) == frm).astype(BF16)


def spread_rows():
    to = lax.broadcasted_iota(jnp.int32, (32, 24), 0)
    frm = lax.broadcasted_iota(jnp.int32, (32, 24), 1)
    return (((frm // 6) * 8 + frm % 6) == to).astype(BF16)


def halves(left, right, odd):
    lane = lax.broadcasted_iota(jnp.int32, left.shape, 1)
    if odd:
        left = pltpu.roll(left, 64, 1)
    else:
        right = pltpu.roll(right, 64, 1)
    return jnp.where(lane < 64, left, right)


class Ledger:
    def __init__(self):
        self.open = {}
        self.seen = set()

    def expect(self, key, wait):
        self.open[key] = wait
        self.seen.add(key)

    def wait(self, *keys):
        for key in keys:
            self.open.pop(key)()

    def finish(self):
        for wait in self.open.values():
            wait()
        self.open = {}


def only(condition, do):
    return lambda: pl.when(condition)(do)


def either(condition, these, others, sem):
    def wait():
        pl.when(condition)(lambda: arrived(these, sem))
        pl.when(jnp.logical_not(condition))(lambda: arrived(others, sem))

    return wait


def layer_kernel(
    tok_hbm, mixg_hbm, qw_hbm, fw_hbm, iw_hbm, lb_hbm, hg_hbm, wo_hbm, st_hbm, ffng_hbm, ids_hbm, wts_hbm,
    gate_ref, up_ref, down_ref, out_ref, st,
    tok, mixg, lb, hg, ffng, ids_ref, wts_ref, wcat, wb, xs, xb, ob, qb, fan, fresh, terms, ro, ho, wob, hb, pb, mb, am_ref, chosen_ref, weight_ref,
    wgu, wd, disp, zr, xg, po, pr, ss, r2, ret, rb,
    lsem, qsem, stsem, wsend, wrecv, xsend, xrecv, osend, orecv, wozs, wozr, woxs, woxr, hsend, hrecv, msend, mrecv,
    lwsem, swsend, swrecv, dsend, drecv, gsend, gu, gv, psend, precv, ssend, srecv, tsend, trecv,
):
    c, z, y, x, u, v = place()
    half = out_ref.shape[1]
    mine = lax.rem(z, 2) == c
    other = 1 - c
    spot = y * 4 + x
    side, row_of = lax.rem(z, 2), z // 2
    pair = [lax.rem(side + i, 2) + 2 * row_of for i in range(2)]
    bar = pltpu.get_barrier_semaphore()
    peers = [{"tp": other}]
    for dz in range(8):
        zk = lax.rem(z + dz, 8)
        for dx in range(4):
            if dz or dx:
                peers.append({"z": zk, "x": lax.rem(x + dx, 4)})
        if dz:
            peers.append({"z": zk, "tp": other})
    for dy in range(1, 4):
        yk = lax.rem(y + dy, 4)
        for dx in range(4):
            peers.append({"y": yk, "x": lax.rem(x + dx, 4)})
        peers.append({"y": yk, "tp": other})
        peers.append({"y": yk, "z": pair[1]})
        peers.append({"y": yk, "z": pair[1], "tp": other})
    for device in peers:
        pl.semaphore_signal(bar, inc=1, device_id=device, device_id_type=MESH_ID)
    loads = [
        pltpu.make_async_copy(a, b, lsem.at[i])
        for i, (a, b) in enumerate(
            ((tok_hbm, tok), (mixg_hbm, mixg), (lb_hbm, lb), (hg_hbm, hg), (ffng_hbm, ffng), (ids_hbm, ids_ref), (wts_hbm, wts_ref),
             (wo_hbm, wob.at[row_of, x]))
        )
    ]
    own = pl.ds(pl.multiple_of(c * 128, 128), 128)
    own_up = pl.ds(pl.multiple_of(256 + c * 128, 128), 128)
    pieces = []
    for i, w_hbm in enumerate((qw_hbm, fw_hbm, iw_hbm)):
        for h in range(4):
            pieces.append(
                pltpu.make_async_copy(w_hbm.at[:, pl.ds(h * 128, 128)], wcat.at[h, :, pl.ds(i * 128, 128)], qsem)
            )
    led = Ledger()
    for i, copy in enumerate(loads[:2] + pieces + loads[2:]):
        copy.start()
    for i, copy in enumerate(loads):
        led.expect(("load", i), copy.wait)
    led.expect("pieces", lambda: arrived(wcat, qsem))
    local = [
        pltpu.make_async_copy(gate_ref.at[0], wgu.at[:, own], lwsem),
        pltpu.make_async_copy(up_ref.at[0], wgu.at[:, own_up], lwsem),
        pltpu.make_async_copy(down_ref.at[0], wd.at[own, :], lwsem),
    ]
    state_in = pltpu.make_async_copy(st_hbm, st, stsem)
    state_in.start()
    led.expect("state", state_in.wait)
    for copy in local:
        copy.start()
    led.expect("local", lambda: arrived(wgu.at[:, pl.ds(0, 384)], lwsem))
    led.wait(("load", 0), ("load", 1))
    tokens = tok[...].astype(F32)
    scale = lax.rsqrt(jnp.mean(tokens * tokens, axis=-1, keepdims=True) + epsilon)
    normed = tokens * scale * mixg[...]
    for yk in range(4):
        for j in range(4):
            a, b = 4 * j + yk // 2, 4 * j + 2 + yk // 2
            xs[yk, :, pl.ds(j * 128, 128)] = halves(
                normed[:, a * 128 : a * 128 + 128], normed[:, b * 128 : b * 128 + 128], yk % 2
            ).astype(BF16)
    led.wait("pieces")
    ones_at = lax.broadcasted_iota(jnp.int32, fan.shape, 0) % 16 == lax.broadcasted_iota(jnp.int32, fan.shape, 1) // 128
    fan[...] = ones_at.astype(BF16)
    zr[...] = jnp.zeros_like(zr)
    rb[...] = jnp.zeros_like(rb)
    pl.semaphore_wait(bar, len(peers))
    out = []
    for dz in (4, 3, 5, 2, 6, 1, 7, 0):
        for dx in (2, 1, 3, 0):
            if dz or dx:
                xk = lax.rem(x + dx, 4)
                out.append(remote(wcat.at[xk], wb.at[z, x], wsend, wrecv, {"z": lax.rem(z + dz, 8), "x": xk}))
    for dy in (2, 1, 3, 0):
        for dx in (2, 1, 3, 0):
            if dy or dx:
                yk = lax.rem(y + dy, 4)
                out.append(remote(xs.at[yk], xb.at[spot], xsend, xrecv, {"y": yk, "x": lax.rem(x + dx, 4)}))
    for copy in out:
        copy.start()
    wbf = wb.reshape(32, 16, 384)
    led.expect("x out", lambda: arrived(xb.at[pl.ds(0, 15)], xsend))
    led.expect("w out", lambda: arrived(wbf.at[pl.ds(0, 31)], wsend))
    led.expect("x", lambda: arrived(xb.at[pl.ds(0, 15)], xrecv))
    led.expect("w", lambda: arrived(wbf.at[pl.ds(0, 31)], wrecv))
    wb[z, x] = wcat[x]
    xb[spot] = xs[y]
    led.wait(*(("load", i) for i in range(2, 8)))
    spread = []
    for k in (4, 2, 6):
        block = wob.at[row_of, x]
        spread.append(remote(block, block, wozs, wozr, {"z": lax.rem(z + k, 8)}))
    for copy in spread:
        copy.start()
    led.expect("woz out", lambda: arrived(xb.at[pl.ds(0, 3)], wozs))
    led.expect("woz", lambda: arrived(xb.at[pl.ds(0, 3)], wozr))
    swap = [
        remote(gate_ref.at[0], wgu.at[:, own], swsend, swrecv, {"tp": other}),
        remote(up_ref.at[0], wgu.at[:, own_up], swsend, swrecv, {"tp": other}),
        remote(down_ref.at[0], wd.at[own, :], swsend, swrecv, {"tp": other}),
    ]
    for copy in swap:
        copy.start()
    led.expect("swap out", lambda: arrived(wgu.at[:, pl.ds(0, 384)], swsend))
    led.expect("swap in", lambda: arrived(wgu.at[:, pl.ds(0, 384)], swrecv))
    chosen, weight = route_slots(ids_ref, wts_ref)
    chosen_ref[...] = chosen.astype(BF16)
    weight_ref[...] = weight
    led.wait("x", "w")
    part = jnp.dot(xb[...].reshape(256, 512), wbf[...].reshape(512, 384), preferred_element_type=F32)
    ob[...] = part.astype(BF16).reshape(16, 16, 384)
    back = []
    for dy in (2, 1, 3, 0):
        for dx in (2, 1, 3, 0):
            if dy or dx:
                yk, xk = lax.rem(y + dy, 4), lax.rem(x + dx, 4)
                back.append(remote(ob.at[yk * 4 + xk], qb.at[spot], osend, orecv, {"y": yk, "x": xk}))
    for copy in back:
        copy.start()
    led.expect("q out", lambda: arrived(qb.at[pl.ds(0, 15)], osend))
    led.expect("q", lambda: arrived(qb.at[pl.ds(0, 15)], orecv))
    qb[spot] = ob[spot]
    led.wait("woz")
    along = []
    for k in (2, 1, 3):
        along.append(remote(wob.at[:, x], wob.at[:, x], woxs, woxr, {"x": lax.rem(x + k, 4)}))
    for copy in along:
        copy.start()
    led.expect("wox out", lambda: arrived(wob.at[:, pl.ds(0, 3)], woxs))
    led.expect("wox", lambda: arrived(wob.at[:, pl.ds(0, 3)], woxr))
    led.wait("state", "q")

    for h in range(4):
        qfv = qb[h].astype(F32) + qb[4 + h].astype(F32) + qb[8 + h].astype(F32) + qb[12 + h].astype(F32)
        bound = lb[h : h + 1, :]
        forget = bound + (1.0 - bound) * (1.0 / (1.0 + jnp.exp(-qfv[:, 128:256])))
        fresh[h] = qfv[:, 256:384]
        for i, value in enumerate((qfv[:, 0:128], forget)):
            upper = value.astype(BF16).astype(F32)
            terms[i, h] = jnp.concatenate([upper, value - upper], axis=0).T.astype(BF16)
    for h in range(4):
        for p in range(8):
            across_lanes = fan[:, 256 * p : 256 * p + 256]
            q_cols = jnp.dot(terms[0, h], across_lanes, preferred_element_type=F32)
            f_cols = jnp.dot(terms[1, h], across_lanes, preferred_element_type=F32)
            for i in range(2):
                s, lanes = 2 * p + i, slice(128 * i, 128 * i + 128)
                row = fresh[h, s : s + 1, :]
                new = row + f_cols[:, lanes] * (st[s, h] - row)
                st[s, h] = new
                ro[h, s : s + 1, :] = jnp.sum(q_cols[:, lanes] * new, axis=0, keepdims=True)
    for h in range(4):
        read = ro[h]
        read = read * lax.rsqrt(jnp.mean(read * read, axis=-1, keepdims=True) + epsilon) * hg[h : h + 1, :]
        ho[:, h * 128 : h * 128 + 128] = read.astype(BF16)
    group = [(k, i) for k in (2, 1, 3, 0) for i in (1, 0)]
    ahead = []
    for k, i in group[:-1]:
        ahead.append(remote(ho, hb.at[side, y], hsend, hrecv, {"y": lax.rem(y + k, 4), "z": pair[i]}))
    for copy in ahead:
        copy.start()
    hbf = hb.reshape(8, 16, 512)
    led.expect("h out", lambda: arrived(hbf.at[pl.ds(0, 7)], hsend))
    led.expect("h", lambda: arrived(hbf.at[pl.ds(0, 7)], hrecv))
    hb[side, y] = ho[...]
    led.wait("wox", "h")
    dims = (((1,), (1,)), ((), ()))
    mixed = lax.dot_general(
        hb[...].reshape(128, 512), wob[...].reshape(256, 512), dims, preferred_element_type=F32
    )
    pb[...] = mixed.astype(BF16).reshape(2, 4, 16, 256)
    home_bound = []
    for k, i in group:
        yk = lax.rem(y + k, 4)
        for t in (0, 1):
            if k or i or t:
                device = {"y": yk, "z": pair[i], "tp": lax.rem(c + t, 2)}
                home_bound.append(remote(pb.at[lax.rem(side + i, 2), yk], mb.at[c, side, y], msend, mrecv, device))
    for copy in home_bound:
        copy.start()
    mbf = mb.reshape(16, 16, 256)
    led.expect("m out", lambda: arrived(mbf.at[pl.ds(0, 15)], msend))
    led.expect("m", lambda: arrived(mbf.at[pl.ds(0, 15)], mrecv))
    mb[c, side, y] = pb[side, y]
    led.wait("m")
    for zk in range(8):
        at = (zk // 4) * 128
        for h in range(2):
            cols = pl.ds(zk * 256 + h * 128, 128)
            left, right = (
                mb[0, zk % 2, k, :, at : at + 128].astype(F32) + mb[1, zk % 2, k, :, at : at + 128].astype(F32)
                for k in (2 * h, 2 * h + 1)
            )
            am_ref[:, cols] = (tok[:, cols].astype(F32) + halves(left, right, zk // 2 % 2)).astype(BF16)
    rows = am_ref[...].astype(F32)
    scale = lax.rsqrt(jnp.mean(rows * rows, axis=-1, keepdims=True) + epsilon)
    ffn_in = (rows * scale * ffng[...]).astype(BF16)
    slots = jnp.dot(chosen_ref[...], ffn_in, preferred_element_type=F32).astype(BF16)
    disp[...] = slots.reshape(disp.shape)
    halves_at = [pl.ds(w * half, half) for w in range(2)]
    for w in range(2):
        for k in (4, 3, 5, 2, 6, 1, 7):
            e = lax.rem(z + k, 8)
            piece = disp.at[e, pl.ds(0, FILLED), halves_at[w]]
            copy = remote(piece, zr.at[w, z // 2, pl.ds(0, FILLED)], dsend, drecv.at[w], {"z": e})

            @pl.when(mine)
            def _(copy=copy):
                copy.start()

        led.expect(("slots", w), either(mine, zr.at[w, pl.ds(0, 3), pl.ds(0, FILLED)], zr.at[w, :, pl.ds(0, FILLED)], drecv.at[w]))
    led.expect("slots out", only(mine, lambda: arrived(disp.at[pl.ds(0, 7), pl.ds(0, FILLED)], dsend)))

    @pl.when(mine)
    def _():
        for w in range(2):
            zr[w, z // 2] = disp[z, :, halves_at[w]]

    lines = [lax.rem(u + j, 4) for j in range(4)]
    across = [lax.rem(v + k, 4) for k in range(4)]
    for w in range(2):
        for j in range(4):
            uj = lines[j]
            if j:
                led.expect(("rows", w, j, 0), lambda w=w, uj=uj: arrived(xg.at[w * 16 + uj * 4 + v], gu.at[w, uj]))
            led.expect(("rows", w, j, 1), lambda w=w, uj=uj: arrived(xg.at[pl.ds(0, 3)], gv.at[w, uj]))
    led.expect("rows out", lambda: arrived(xg.at[pl.ds(0, 30)], gsend))
    led.expect("parts out", lambda: arrived(xg.at[pl.ds(0, 24)], psend))
    led.expect("sums out", lambda: arrived(xg.at[pl.ds(0, 6)], ssend))

    def along_v(w, j):
        block = xg.at[w * 16 + lines[j] * 4 + v]
        for k in (2, 1, 3):
            remote(block, block, gsend, gv.at[w, lines[j]], plane_id(c, u, across[k])).start()

    def from_z(w):
        led.wait(("slots", w))
        packed = jnp.dot(squeeze_rows(), zr[w].reshape(32, half), preferred_element_type=F32).astype(BF16)
        xg[w * 16 + u * 4 + v] = packed
        block = xg.at[w * 16 + u * 4 + v]
        for k in (1, 3, 2):
            remote(block, block, gsend, gu.at[w, u], plane_id(c, lines[k], v)).start()
        along_v(w, 0)

    def from_u(w, j):
        led.wait(("rows", w, j, 0))
        along_v(w, j)

    def first(w, j):
        led.wait(("rows", w, j, 1))
        rows_in = xg[pl.ds(w * 16 + lines[j] * 4, 4)].reshape(96, half)
        return jnp.dot(rows_in, wgu[halves_at[w], :], preferred_element_type=F32)

    def reduce_v(w, j):
        uj = lines[j]
        for k in (2, 1, 3):
            there = plane_id(c, u, across[k])
            remote(po.at[w, uj, across[k]], pr.at[w, uj, v], psend, precv.at[w, uj], there).start()
        led.expect(("part in", w, j), lambda: arrived(pr.at[w, uj, pl.ds(0, 3)], precv.at[w, uj]))

    def second(j):
        uj = lines[j]
        pre = first(0, j) + first(1, j)
        gate_pre, up_pre = pre[:, :256], pre[:, 256:]
        hidden = (gate_pre / (1.0 + jnp.exp(-gate_pre)) * up_pre).astype(BF16)
        for w in range(2):
            part = jnp.dot(hidden, wd[:, halves_at[w]], preferred_element_type=F32).astype(BF16)
            po[w, uj] = part.reshape(4, 24, half)
            if j:
                reduce_v(w, j)

    def gather(w, j):
        uj = lines[j]
        led.wait(("part in", w, j))
        total = po[w, uj, v].astype(F32)
        for k in (1, 3, 2):
            total += pr[w, uj, across[k]].astype(F32)
        return total

    def hand_over(w, j):
        uj = lines[j]
        ss[w, uj] = gather(w, j).astype(BF16)
        remote(ss.at[w, uj], r2.at[w, u], ssend, srecv.at[w], plane_id(c, uj, v)).start()

    def give_back(w):
        total = gather(w, 0)
        arrived(r2.at[w, pl.ds(0, 3)], srecv.at[w])
        for k in (1, 3, 2):
            total += r2[w, lines[k]].astype(F32)
        ret[:, :, halves_at[w]] = (
            jnp.dot(spread_rows(), total.astype(BF16), preferred_element_type=F32).astype(BF16).reshape(4, 8, half)
        )
        for k in (2, 1, 3, 0):
            at = lax.rem(z // 2 + k, 4)
            zk = 2 * at + c
            piece = ret.at[at, pl.ds(0, FILLED), halves_at[w]]
            copy = remote(piece, rb.at[z, pl.ds(0, FILLED)], tsend, trecv, {"z": zk, "tp": w})
            away = jnp.logical_or(zk != z, c != w)

            @pl.when(away)
            def _(copy=copy):
                copy.start()


    from_z(0)
    from_z(1)
    led.wait("local", "swap in")
    from_u(0, 3)
    from_u(0, 1)
    from_u(0, 2)
    from_u(1, 3)
    from_u(1, 1)
    from_u(1, 2)
    second(0)
    second(3)
    second(1)
    second(2)
    reduce_v(0, 0)
    reduce_v(1, 0)
    for j in (3, 1, 2):
        for w in range(2):
            hand_over(w, j)
    give_back(0)
    give_back(1)

    @pl.when(mine)
    def _():
        rb[z] = ret[z // 2, :, pl.ds(pl.multiple_of(c * half, half), half)]

    seven, eight = rb.at[pl.ds(0, 7), pl.ds(0, FILLED)], rb.at[:, pl.ds(0, FILLED)]
    either(mine, seven, eight, trecv)()
    led.expect("returned out", either(mine, seven, eight, tsend))
    returned = rb[...].reshape(64, half)
    weight = weight_ref[...]
    upper = weight.astype(BF16)
    lower = (weight - upper.astype(F32)).astype(BF16)
    dims = (((0,), (0,)), ((), ()))
    mix = lax.dot_general(upper, returned, dims, preferred_element_type=F32)
    mix += lax.dot_general(lower, returned, dims, preferred_element_type=F32)
    keep = am_ref[:, pl.ds(pl.multiple_of(c * half, half), half)].astype(F32)
    out_ref[...] = (keep + mix).astype(BF16)
    led.finish()


NPIECE = 4


def emit_kernel(mixed_ref, state_ref, mixed_out, state_out, sem):
    step = 16 // NPIECE
    copies = [
        pltpu.make_async_copy(state_ref.at[pl.ds(i * step, step)], state_out.at[pl.ds(i * step, step)], sem.at[i])
        for i in range(NPIECE)
    ]
    copies.append(pltpu.make_async_copy(mixed_ref, mixed_out, sem.at[NPIECE]))
    for copy in copies:
        copy.start()
    for copy in copies:
        copy.wait()


def shards(
    tokens, mix_gain, query_weight, forget_weight, input_weight, lower_bound, head_gain, out_weight, state,
    ffn_gain, route_ids, route_weights, expert_gate, expert_up, expert_down,
):
    rows, width = tokens.shape
    half = width // 2
    hbm = pl.BlockSpec(memory_space=pltpu.HBM)
    vmem = pl.BlockSpec(memory_space=pltpu.VMEM)
    dma = pltpu.SemaphoreType.DMA
    scratch = lambda *shape, dtype=BF16: pltpu.VMEM(shape, dtype)
    held = lambda a: pltpu.with_memory_space_constraint(a, pltpu.HBM)
    mixed_out, new_state = pl.pallas_call(
        layer_kernel,
        out_shape=(pltpu.VMEM((rows, half), BF16), pltpu.VMEM(state.shape, F32)),
        in_specs=[hbm] * 15,
        out_specs=(vmem, vmem),
        scratch_shapes=[
            scratch(rows, width), scratch(1, width, dtype=F32), scratch(4, 128, dtype=F32), scratch(4, 128, dtype=F32),
            scratch(1, width, dtype=F32), scratch(2, 16, dtype=jnp.int32), scratch(2, 16, dtype=F32),
            scratch(4, 16, 384), scratch(8, 4, 16, 384), scratch(4, 16, 512), scratch(16, 16, 512),
            scratch(16, 16, 384), scratch(16, 16, 384), scratch(32, width), scratch(4, 16, 128, dtype=F32),
            scratch(2, 4, 128, 32), scratch(4, 16, 128, dtype=F32),
            scratch(16, 512), scratch(4, 4, 16, 512), scratch(2, 4, 16, 512), scratch(2, 4, 16, 256), scratch(2, 2, 4, 16, 256),
            scratch(rows, width), scratch(64, 16), scratch(64, 16, dtype=F32),
            scratch(width, 512), scratch(256, width), scratch(8, 8, width), scratch(2, 4, 8, half),
            scratch(32, 24, half), scratch(2, 4, 4, 24, half), scratch(2, 4, 4, 24, half), scratch(2, 4, 24, half),
            scratch(2, 4, 24, half),
            scratch(4, 8, width), scratch(8, 8, half),
            dma((8,)), *[dma] * 16,
            *[dma] * 3, dma, dma((2,)), dma, dma((2, 4)), dma((2, 4)), dma, dma((2, 4)), dma, dma((2,)), dma, dma,
        ],
        compiler_params=pltpu.CompilerParams(
            collective_id=0, has_side_effects=True, vmem_limit_bytes=48 * 2**20
        ),
        name="layer",
    )(
        *map(held, (
            tokens, mix_gain.reshape(1, -1), query_weight, forget_weight, input_weight, lower_bound.reshape(4, 128),
            head_gain.reshape(4, 128), out_weight.T, state, ffn_gain.reshape(1, -1), route_ids.T, route_weights.T,
            expert_gate, expert_up, expert_down,
        ))
    )
    return pl.pallas_call(
        emit_kernel,
        out_shape=(pltpu.HBM(mixed_out.shape, BF16), pltpu.HBM(state.shape, F32)),
        in_specs=[pl.BlockSpec(memory_space=pltpu.VMEM)] * 2,
        out_specs=(hbm, hbm),
        scratch_shapes=[dma((NPIECE + 1,))],
        compiler_params=pltpu.CompilerParams(vmem_limit_bytes=4 * 2**20),
        name="emit",
    )(*(pltpu.with_memory_space_constraint(a, pltpu.VMEM) for a in (mixed_out, new_state)))


def solution(mesh):
    finer = Mesh(mesh.devices.reshape(8, 4, 4, mesh.shape["tp"]), ("z", "y", "x", "tp"))
    placed = (
        P(EP, None), P(), P(EP, "tp"), P(EP, "tp"), P(EP, "tp"), P("tp"), P("tp"), P("tp", EP),
        P(EP, "tp", None, None), P(), P(EP, None), P(EP, None), P(EP, None, "tp"), P(EP, None, "tp"), P(EP, "tp", None),
    )
    return jax.shard_map(
        shards, mesh=finer, in_specs=placed, out_specs=(P(EP, "tp"), P(EP, "tp", None, None)), check_vma=False
    )
```
